1024 devices in a mesh: ep: 64 (over z, core), tp: 16 (over y, x).
Axes of the slice: x: 4, y: 4, z: 32, core: 2. Of those that a mesh axis runs over, the one named last changes fastest.
Arguments:
- tokens: bfloat16 [768, 4096], P('ep', 'tp')
- norm_gain: float32 [4096], P('tp'), may hold values from 0.1 to 1.9
- routes: int32 [768, 6], P('ep'), may hold values from 0 to 63, all different within a row; in each aligned block of 12 rows (0 to 11, 12 to 23, ...) at most 2 rows name the same one
- route_weights: float32 [768, 6], P('ep'), may hold values from 0.05 to 1
- expert_gate: bfloat16 [64, 4096, 1024], P('ep', 'tp'), may hold values from -0.09375 to 0.09375
- expert_up: bfloat16 [64, 4096, 1024], P('ep', 'tp'), may hold values from -0.09375 to 0.09375
- expert_down: bfloat16 [64, 1024, 4096], P('ep', None, 'tp'), may hold values from -0.1875 to 0.1875
- shared_gate: bfloat16 [4096, 1024], P('tp'), may hold values from -0.09375 to 0.09375
- shared_up: bfloat16 [4096, 1024], P('tp'), may hold values from -0.09375 to 0.09375
- shared_down: bfloat16 [1024, 4096], P(None, 'tp'), may hold values from -0.1875 to 0.1875
Outputs:
- mixed: bfloat16 [768, 4096], P('ep', 'tp')
The draws below stay inside these ranges and needn't reach their ends.
Inputs may be any that keep to these rules, and one draw needn't show every extreme that they name: `routes`: each row names 6 different experts; among the rows of one device no expert is named more than 2 times, and in some devices' rows one expert is named exactly 2 times.
All inputs are finite; a program needn't handle non-finite values.
Results may differ from the reference program's by a relative error of at most 0.0068.
Values may be sent and summed in bfloat16 or wider, within the bound.
A program may use at most 32 MiB of HBM per device.

```python
import math
import jax
import jax.numpy as jnp
import numpy as np
from jax import lax

D = 4096
FF_E = 1024
FF_S = 1024
TOP_K = 6
TOK_DEV = 12
EXPERTS = 64
CAP = 2
TOKENS = 768
N_EP = 64


def draw_tokens(key, part):
    first, second = jax.random.split(jax.random.fold_in(key, 11), 2)
    column = jnp.arange(D, dtype=jnp.float32) / D
    rising = jnp.exp(jnp.log(8.0) * column)[None, :]
    base = jax.random.normal(first, (TOKENS, D), jnp.float32)
    rough = jax.random.uniform(second, (1, D), jnp.float32, 0.5, 1.5)
    values = jnp.clip(base, -6.0, 6.0) * rough * rising
    return values.astype(jnp.bfloat16)


def block_levels(key, shape, cuts, least, high):
    def one(dim, parts):
        steps = jax.random.uniform(jax.random.fold_in(jax.random.fold_in(key, 6), dim), (parts,), jnp.float32, least / len(cuts), high / len(cuts))
        return jnp.repeat(jnp.exp(steps), shape[dim] // parts).reshape((-1,) + (1,) * (len(shape) - dim - 1))

    level = one(*cuts[0])
    for cut in cuts[1:]:
        level = level * one(*cut)
    return level


def deal_out(stream_key, own, number, rows, count, top, limit, lean):
    sequence = jax.random.permutation(stream_key, count)
    heavy_load, common = shares(count, rows * top, limit, lean, True), shares(count, rows * top, limit, lean, False)
    places = jnp.arange(count)

    def named(tallies, offset_by):
        used = int((tallies > 0).sum())
        fixed = max(1, used // 4)
        moved = fixed + (places - fixed + offset_by * (used - fixed)) % max(1, count - fixed)
        return jnp.zeros((count,), jnp.int32).at[sequence[jnp.where(places < fixed, places, moved)]].set(jnp.asarray(tallies, jnp.int32))

    tallies = jnp.where(number % 4 == 0, named(heavy_load, number // 4), named(common, number - number // 4 - 1))
    mixed = jax.random.permutation(jax.random.fold_in(own, 3), count)
    donor, receiver = mixed[0:count // 2 * 2:2], mixed[1:count // 2 * 2:2]
    room = jnp.minimum(tallies[donor] - 1, limit - tallies[receiver]) // 2
    room = jnp.where((donor == sequence[0]) | (receiver == sequence[0]) | (tallies[receiver] == 0), 0, jnp.maximum(room, 0))
    moved = jax.random.randint(jax.random.fold_in(own, 4), (count // 2,), 0, 1 << 20) % (room + 1)
    tallies = tallies.at[donor].add(-moved).at[receiver].add(moved)
    labels = jnp.searchsorted(jnp.cumsum(tallies), jnp.arange(rows * top), side="right").astype(jnp.int32)
    grid = labels.reshape(top, rows).T
    grid = grid[jax.random.permutation(jax.random.fold_in(own, 1), rows)]
    offset_by = jax.random.randint(jax.random.fold_in(own, 2), (rows, 1), 0, top)
    return jnp.take_along_axis(grid, (jnp.arange(top)[None, :] + offset_by) % top, axis=1)


def shares(count, total, most, slope, full):
    weights = [(1 << 20) // math.isqrt(rank ** slope) + 1 for rank in range(1, count + 1)]
    largest = most if full else min(most, max(-(-total // count), total * weights[0] // sum(weights)))
    least = 1 if total - largest >= count - 1 else 0
    given, spare = [largest] + [least] * (count - 1), total - largest - least * (count - 1)
    while spare > 0:
        free = [i for i in range(1, count) if given[i] < largest] or [i for i in range(1, count) if given[i] < most]
        whole, budget = sum([weights[i] for i in free]), spare
        for i in free:
            addition = min(most - given[i], max(1, budget * weights[i] // whole), spare)
            given[i] = given[i] + addition
            spare = spare - addition
    return np.array(given)


def normal_values(own_key, dims, width, bound, cuts=(), held_as=jnp.bfloat16):
    entries = jax.random.normal(own_key, dims, jnp.float32) * width
    if len(cuts) > 0:
        entries = block_levels(own_key, dims, cuts, -0.22, 0.18) * entries
    return jnp.clip(entries, min=-bound, max=bound).astype(held_as)


def setup_inputs(seed: int = 0) -> dict:
    streams_of = jax.random.split(jax.random.key(seed), 11)
    tokens = draw_tokens(jax.random.fold_in(streams_of[10], 71), 0)
    norm_gain = jnp.clip(1.0 + 0.18 * jax.random.normal(streams_of[1], (D,), jnp.float32), 0.1, 1.9)
    routes_keys = jax.random.split(jax.random.fold_in(streams_of[2], 1), TOKENS // TOK_DEV)
    routes_turns = jax.random.permutation(jax.random.fold_in(streams_of[2], 3), TOKENS // TOK_DEV)
    routes = jax.vmap(lambda own, number: deal_out(jax.random.fold_in(streams_of[2], 2), own, number, TOK_DEV, EXPERTS, TOP_K, CAP, 2))(routes_keys, routes_turns).reshape((TOKENS, TOP_K))
    route_weights = jnp.clip(jnp.exp(math.log(1.0) - 2.9957323 * jax.random.uniform(streams_of[3], (TOKENS, TOP_K), jnp.float32) ** block_levels(streams_of[3], (TOKENS, TOP_K), ((0, 64),), -0.2, 0.2)), 0.05, 1.0)
    expert_gate = normal_values(streams_of[4], (EXPERTS, D, FF_E), D ** -0.5, 0.09375, ((0, 64), (1, 16)))
    expert_up = normal_values(streams_of[5], (EXPERTS, D, FF_E), D ** -0.5, 0.09375, ((0, 64), (1, 16)))
    expert_down = normal_values(streams_of[6], (EXPERTS, FF_E, D), FF_E ** -0.5, 0.1875, ((0, 64), (2, 16)))
    shared_gate = normal_values(streams_of[7], (D, FF_S), D ** -0.5, 0.09375, ((0, 16),))
    shared_up = normal_values(streams_of[8], (D, FF_S), D ** -0.5, 0.09375, ((0, 16),))
    shared_down = normal_values(streams_of[9], (FF_S, D), FF_S ** -0.5, 0.1875, ((1, 16),))
    return {"tokens": tokens, "norm_gain": norm_gain, "routes": routes, "route_weights": route_weights, "expert_gate": expert_gate, "expert_up": expert_up, "expert_down": expert_down, "shared_gate": shared_gate, "shared_up": shared_up, "shared_down": shared_down}


def block_ranks(route_blocks, n_experts):
    onehot = (route_blocks[..., None] == jnp.arange(n_experts, dtype=jnp.int32)).astype(jnp.int32)
    before = jnp.cumsum(onehot, axis=1) - onehot
    return lax.optimization_barrier(jnp.sum(before * onehot, axis=-1))

def expert_tables(route_blocks, weight_blocks, expert, capacity, n_experts):
    blocks, tok, picks = route_blocks.shape
    ranks = block_ranks(route_blocks.reshape(blocks, tok * picks), n_experts).reshape(blocks, tok, picks)
    slot = jnp.where(route_blocks == expert, ranks, -1)
    hits = slot[..., None] == jnp.arange(capacity, dtype=jnp.int32)
    select = jnp.any(hits, axis=2).astype(jnp.float32)
    weighted = lax.optimization_barrier(jnp.sum(jnp.where(hits, weight_blocks[..., None], 0.0), axis=2))
    return (select, weighted)

def swiglu(rows, gate_w, up_w, down_w):
    gate = jnp.dot(rows, gate_w, preferred_element_type=jnp.float32)
    up = jnp.dot(rows, up_w, preferred_element_type=jnp.float32)
    hidden = (jax.nn.silu(gate) * up).astype(jnp.bfloat16)
    return jnp.dot(hidden, down_w, preferred_element_type=jnp.float32)

def reference(tokens, norm_gain, routes, route_weights, expert_gate, expert_up, expert_down, shared_gate, shared_up, shared_down):
    values = tokens.astype(jnp.float32)
    meansq = lax.optimization_barrier(jnp.mean(values * values, axis=1, keepdims=True))
    normed = (values * lax.rsqrt(meansq + 1e-06) * norm_gain.astype(jnp.float32)[None, :]).astype(jnp.bfloat16)
    scaled = 2.5 * route_weights / lax.optimization_barrier(jnp.sum(route_weights, axis=1, keepdims=True))
    shared_out = swiglu(normed, shared_gate, shared_up, shared_down)
    capacity = max(2, TOK_DEV * TOP_K // N_EP + 1)
    route_blocks = routes.reshape(N_EP, TOK_DEV, TOP_K)
    weight_blocks = scaled.reshape(N_EP, TOK_DEV, TOP_K)
    x_blocks = normed.reshape(N_EP, TOK_DEV, D).astype(jnp.float32)

    def one_expert(carry, packed):
        gate_w, up_w, down_w, expert = packed
        select, weighted = expert_tables(route_blocks, weight_blocks, expert, capacity, EXPERTS)
        rows = jnp.einsum('stc,std->scd', select, x_blocks).astype(jnp.bfloat16)
        result = swiglu(rows.reshape(N_EP * capacity, D), gate_w, up_w, down_w).astype(jnp.bfloat16)
        result = result.reshape(N_EP, capacity, D).astype(jnp.float32)
        carry = carry + jnp.einsum('stc,scd->std', weighted, result, precision=lax.Precision.HIGHEST)
        return (carry, None)
    start = jnp.zeros((N_EP, TOK_DEV, D), jnp.float32)
    routed, _ = lax.scan(one_expert, start, (expert_gate, expert_up, expert_down, jnp.arange(EXPERTS, dtype=jnp.int32)))
    return (shared_out + routed.reshape(TOKENS, D)).astype(jnp.bfloat16)
```

```python
import functools

import jax
import jax.numpy as jnp
from jax import lax
from jax.experimental import pallas as pl
from jax.experimental.pallas import tpu as pltpu
from jax.sharding import Mesh
from jax.sharding import PartitionSpec as P

MESH = pl.DeviceIdType.MESH
F32 = jnp.float32
BF16 = jnp.bfloat16
DOWN_SCALE = 2.0**-40
UP_SCALE = 2.0**40


def silu(v):
    return v / (1.0 + jnp.exp(-v))


def row_of(col, width):
    rows = col.shape[0]
    eye = lax.broadcasted_iota(jnp.int32, (rows, width), 0) == lax.broadcasted_iota(
        jnp.int32, (rows, width), 1
    )
    return jnp.sum(jnp.where(eye, col, 0.0), axis=0, keepdims=True)


def col_of(row, rows, first):
    width = row.shape[1]
    eye = lax.broadcasted_iota(jnp.int32, (rows, width), 0) + first == lax.broadcasted_iota(
        jnp.int32, (rows, width), 1
    )
    return jnp.sum(jnp.where(eye, row, 0.0), axis=1, keepdims=True)


def kernel(
    sizes,
    tok_hbm,
    gain_hbm,
    routes_hbm,
    weights_hbm,
    eg_hbm,
    eu_hbm,
    ed_hbm,
    sg_hbm,
    su_hbm,
    sd_hbm,
    out_ref,
    tok,
    gain,
    routes,
    weights,
    eg,
    eu,
    ed,
    sg,
    su,
    sd,
    tok16,
    routes16,
    weights16,
    slotw,
    shared_out,
    msg,
    relay_p,
    relay_m,
    rx,
    sq_tx,
    sq_rx,
    sqs_tx,
    sqs_rx,
    part_tx,
    part_rx,
    spart_tx,
    spart_rx,
    hid_tx,
    hid,
    shid_tx,
    shid,
    ret,
    back,
    load_sem,
    disp_send,
    disp_recv,
    rel_send,
    rel_recv,
    tp_send,
    sq_recv,
    part_recv,
    hid_recv,
    ret_send,
    ret_recv,
):
    nz, ny, nx, hop = sizes
    ntp = ny * nx
    half_z = nz // 2
    tok_n, picks = routes.shape
    width = tok.shape[1]
    total_width = float(width * ntp)
    slots = 4 * nz
    rows = slots // 2
    half = rows // 2
    ff = eg.shape[1]
    chunk = ff // (ntp // 2)
    n_plus, n_minus = half_z - 1 - hop, half_z - hop

    z, c = lax.axis_index("z"), lax.axis_index("c")
    y, x = lax.axis_index("y"), lax.axis_index("x")
    me = y * nx + x
    my_half, my_chunk = lax.rem(me, 2), me // 2

    def at(d):
        return lax.rem(z + d + 2 * nz, nz)

    def peer(i):
        j = lax.rem(me + i, ntp)
        return j, (z, c, j // nx, lax.rem(j, nx))

    loads = []
    for i, (src, dst) in enumerate(
        (
            (tok_hbm, tok),
            (routes_hbm, routes),
            (weights_hbm, weights),
            (gain_hbm, gain),
            (sg_hbm, sg),
            (su_hbm, su),
            (eg_hbm.at[0], eg),
            (eu_hbm.at[0], eu),
            (sd_hbm, sd),
            (ed_hbm.at[0], ed),
        )
    ):
        copy = pltpu.make_async_copy(src, dst, load_sem.at[i])
        copy.start()
        loads.append(copy)

    barrier = pltpu.get_barrier_semaphore()

    def greet_z(d, carry):
        for core in range(2):
            pl.semaphore_signal(barrier, inc=1, device_id=(at(d), core, y, x), device_id_type=MESH)
            pl.semaphore_signal(barrier, inc=1, device_id=(at(-d), core, y, x), device_id_type=MESH)
        return carry

    def greet_tp(i, carry):
        pl.semaphore_signal(barrier, inc=1, device_id=peer(i)[1], device_id_type=MESH)
        return carry

    lax.fori_loop(1, hop + 1, greet_z, 0)
    pl.semaphore_signal(barrier, inc=1, device_id=(z, 1 - c, y, x), device_id_type=MESH)
    lax.fori_loop(1, ntp, greet_tp, 0)

    tok16[...] = jnp.zeros_like(tok16)
    routes16[...] = jnp.full_like(routes16, -1)
    weights16[...] = jnp.ones_like(weights16)
    for i in range(4):
        loads[i].wait()
    tok16[0:tok_n, :] = tok[...]
    routes16[0:tok_n, :] = routes[...]
    weights16[0:tok_n, :] = weights[...]
    picked, affinity = routes16[...], weights16[...]
    lane = lax.broadcasted_iota(jnp.int32, (16, slots), 1)
    chip = lane // 4 + (z + half_z)
    chip = jnp.where(chip >= nz, chip - nz, chip)
    chip = jnp.where(chip >= nz, chip - nz, chip)
    expert = chip * 2 + (lane // 2) % 2
    scaled = 2.5 * affinity / jnp.sum(affinity, axis=1, keepdims=True)
    named = jnp.zeros((16, slots), F32)
    weight = jnp.zeros((16, slots), F32)
    for k in range(picks):
        hit = picked[:, k : k + 1] == expert
        named = jnp.where(hit, 1.0, named)
        weight = jnp.where(hit, scaled[:, k : k + 1], weight)
    earlier = (
        lax.broadcasted_iota(jnp.int32, (16, 16), 1) < lax.broadcasted_iota(jnp.int32, (16, 16), 0)
    ).astype(F32)
    before = jnp.dot(earlier, named, preferred_element_type=F32)
    rank = (lane % 2).astype(F32)
    select = jnp.where(before == rank, named, 0.0)
    slotw[...] = jnp.where(before == rank, weight, 0.0)
    tokens16 = tok16[...]
    outgoing = lax.dot_general(
        select.astype(BF16), tokens16, (((0,), (0,)), ((), ())), preferred_element_type=F32
    ).astype(BF16)
    for i in range(slots // 2):
        msg[i] = outgoing[2 * i : 2 * i + 2, :]

    gains = gain[...] * DOWN_SCALE
    values = tokens16.astype(F32)
    scaled_tok = (values * gains).astype(BF16)
    sqs_tx[...] = row_of(jnp.sum(values * values, axis=1, keepdims=True), 128)
    sqs_rx[me] = sqs_tx[...]

    pl.semaphore_wait(barrier, 4 * hop + 1 + ntp - 1)

    def bundle(first, count, landing, target, k):
        return pltpu.make_async_remote_copy(
            src_ref=msg.at[pl.ds(first, count)],
            dst_ref=landing.at[:, c],
            send_sem=disp_send,
            recv_sem=rel_recv.at[k],
            device_id=(target, 1, y, x),
            device_id_type=MESH,
        )

    bundle(2 * (half_z + hop + 1), 2 * n_plus, relay_p, at(hop), 0).start()
    bundle(0, 2 * n_minus, relay_m, at(-hop), 1).start()

    def place(d):
        p = lax.rem(hop - d + 2 * nz, nz)
        return p // half_z, lax.rem(p, half_z)

    def send_near(d, core):
        group, p = place(d)
        pltpu.make_async_remote_copy(
            src_ref=msg.at[2 * (d + half_z) + core],
            dst_ref=rx.at[group, 2 * p + c],
            send_sem=disp_send,
            recv_sem=disp_recv.at[group],
            device_id=(at(d), core, y, x),
            device_id_type=MESH,
        ).start()

    def near(i, carry):
        d = hop - i
        for core in range(2):
            send_near(d, core)
            send_near(-d, core)
        return carry

    lax.fori_loop(0, hop, near, 0)
    send_near(0, 1 - c)
    g0, p0 = place(0)
    rx[g0, 2 * p0 + c] = msg[2 * half_z + c]

    def to_tp(src, dst, recv):
        def one(i, carry):
            j, device = peer(i)
            pltpu.make_async_remote_copy(
                src_ref=src(j),
                dst_ref=dst,
                send_sem=tp_send,
                recv_sem=recv,
                device_id=device,
                device_id_type=MESH,
            ).start()
            return carry

        lax.fori_loop(1, ntp, one, 0)

    def waiting(src, dst, send, recv):
        return pltpu.make_async_remote_copy(
            src_ref=src,
            dst_ref=dst,
            send_sem=send,
            recv_sem=recv,
            device_id=peer(1)[1],
            device_id_type=MESH,
        )

    to_tp(lambda j: sqs_tx, sqs_rx.at[me], sq_recv.at[2])
    for i in (4, 5):
        loads[i].wait()
    for n, w in enumerate((sg, su)):
        part = jnp.dot(scaled_tok, w[...], preferred_element_type=F32)
        for k in range(ntp // 2):
            for h in range(2):
                spart_tx[2 * k + h, n] = part[8 * h : 8 * h + 8, k * chunk : (k + 1) * chunk]
    to_tp(lambda j: spart_tx.at[j], spart_rx.at[me], part_recv.at[2])
    spart_rx[me] = spart_tx[me]

    @pl.when(c == 1)
    def _():
        waiting(relay_p, relay_p, rel_send, rel_recv.at[0]).wait_recv()

        def forward_plus(i, carry):
            for core in range(2):
                group, p = place(i + hop + 1)
                pltpu.make_async_remote_copy(
                    src_ref=relay_p.at[2 * i + core],
                    dst_ref=rx.at[group, pl.ds(2 * p, 2)],
                    send_sem=rel_send,
                    recv_sem=disp_recv.at[group],
                    device_id=(at(i + 1), core, y, x),
                    device_id_type=MESH,
                ).start()
            return carry

        lax.fori_loop(0, n_plus, forward_plus, 0)
        waiting(relay_m, relay_m, rel_send, rel_recv.at[1]).wait_recv()

        def forward_minus(i, carry):
            for core in range(2):
                group, p = place(i - half_z)
                pltpu.make_async_remote_copy(
                    src_ref=relay_m.at[2 * i + core],
                    dst_ref=rx.at[group, pl.ds(2 * p, 2)],
                    send_sem=rel_send,
                    recv_sem=disp_recv.at[group],
                    device_id=(at(i - half_z + hop), core, y, x),
                    device_id_type=MESH,
                ).start()
            return carry

        lax.fori_loop(0, n_minus, forward_minus, 0)

    def gate_up(group):
        count = 2 * half_z - (1 if group == 0 else 0)
        arrived = rx.at[group, pl.ds(0, count)]
        waiting(arrived, arrived, disp_send, disp_recv.at[group]).wait_recv()
        values = rx[group].reshape(rows, width).astype(F32)
        sq_tx[group] = row_of(jnp.sum(values * values, axis=1, keepdims=True), 128)
        sq_rx[group, me] = sq_tx[group]
        to_tp(lambda j: sq_tx.at[group], sq_rx.at[group, me], sq_recv.at[group])
        lhs = (values * gains).astype(BF16)
        for n, w in enumerate((eg, eu)):
            part = jnp.dot(lhs, w[...], preferred_element_type=F32).astype(BF16)
            for k in range(ntp // 2):
                for h in range(2):
                    part_tx[group, 2 * k + h, n] = part[
                        half * h : half * (h + 1), k * chunk : (k + 1) * chunk
                    ]
        to_tp(lambda j: part_tx.at[group, j], part_rx.at[group, me], part_recv.at[group])
        part_rx[group, me] = part_tx[group, me]

    def hidden_of(squares, parts, n):
        total = jnp.zeros((1, 128), F32)
        gate = jnp.zeros((n, chunk), F32)
        up = jnp.zeros((n, chunk), F32)
        for j in range(ntp):
            total = total + squares[j]
            gate = gate + parts[j, 0].astype(F32)
            up = up + parts[j, 1].astype(F32)
        inv = lax.rsqrt(total / total_width + 1e-06) * UP_SCALE
        inv = col_of(inv, n, my_half * n)
        return (silu(gate * inv) * (up * inv)).astype(BF16)

    def tp_wait(buf, recv):
        some = buf.at[pl.ds(0, ntp - 1)]
        waiting(some, some, tp_send, recv).wait_recv()

    columns = pl.ds(pl.multiple_of(my_chunk * chunk, chunk), chunk)

    def reduce_group(group):
        tp_wait(sq_rx.at[group], sq_recv.at[group])
        tp_wait(part_rx.at[group], part_recv.at[group])
        hid_tx[group] = hidden_of(sq_rx.at[group], part_rx.at[group], half)
        own = hid.at[group, pl.ds(pl.multiple_of(my_half * half, half), half), columns]
        own[...] = hid_tx[group]
        to_tp(lambda j: hid_tx.at[group], own, hid_recv.at[group])

    def reduce_shared():
        tp_wait(sqs_rx, sq_recv.at[2])
        tp_wait(spart_rx, part_recv.at[2])
        shid_tx[...] = hidden_of(sqs_rx, spart_rx, 8)
        own = shid.at[my_half, :, columns]
        own[...] = shid_tx[...]
        to_tp(lambda j: shid_tx, own, hid_recv.at[2])

    def down_shared():
        waiting(spart_half, spart_half, tp_send, hid_recv.at[2]).wait_recv()
        loads[8].wait()
        total = jnp.zeros((16, width), F32)
        hidden = jnp.concatenate([shid[0], shid[1]], axis=0)
        shared_out[...] = total + jnp.dot(hidden, sd[...], preferred_element_type=F32)

    spart_half = part_rx.at[0, pl.ds(0, ntp - 1), 0, pl.ds(0, 8)]

    def down(group):
        blocks = part_rx.at[group, pl.ds(0, ntp - 1), 0]
        waiting(blocks, blocks, tp_send, hid_recv.at[group]).wait_recv()
        result = jnp.dot(hid[group], ed[...], preferred_element_type=F32).astype(BF16)
        for i in range(rows // 2):
            ret[group, i] = result[2 * i : 2 * i + 2, :]

        def give_back(p):
            s = p - hop
            place_there = 2 * lax.rem(half_z - s + 2 * nz, nz) + c
            for core in range(2):
                pltpu.make_async_remote_copy(
                    src_ref=ret.at[group, 2 * (p - group * half_z) + core],
                    dst_ref=back.at[place_there],
                    send_sem=ret_send,
                    recv_sem=ret_recv,
                    device_id=(at(s), core, y, x),
                    device_id_type=MESH,
                ).start()

        if group == 0:

            def outer(i, carry):
                give_back(i)
                give_back(half_z - 1 - i)
                return carry

            lax.fori_loop(0, hop - 1, outer, 0)
            give_back(hop - 1)
            pltpu.make_async_remote_copy(
                src_ref=ret.at[0, 2 * hop + 1 - c],
                dst_ref=back.at[2 * half_z + c],
                send_sem=ret_send,
                recv_sem=ret_recv,
                device_id=(z, 1 - c, y, x),
                device_id_type=MESH,
            ).start()
            back[2 * half_z + c] = ret[0, 2 * hop + c]
        else:
            farthest = half_z + hop

            def inner(i, carry):
                give_back(farthest - i)
                give_back(farthest + 1 + i)
                return carry

            give_back(half_z)
            lax.fori_loop(0, hop - 1, inner, 0)
            give_back(half_z + 1)

    for i in (6, 7):
        loads[i].wait()
    gate_up(0)
    reduce_shared()
    gate_up(1)
    reduce_group(0)
    down_shared()
    loads[9].wait()
    reduce_group(1)
    down(0)
    down(1)

    got = back.at[pl.ds(0, 2 * nz - 1)]
    waiting(got, got, ret_send, ret_recv).wait_recv()
    rows_back = back[...].reshape(slots, width).astype(F32)
    routed = jnp.dot(
        slotw[...], rows_back, precision=lax.Precision.HIGHEST, preferred_element_type=F32
    )
    out_ref[...] = (shared_out[...] + routed)[0:tok_n, :].astype(BF16)

    def left(ref, sem):
        waiting(ref, ref, sem, ret_recv).wait_send()

    left(got, ret_send)
    left(msg.at[pl.ds(0, 2 * (n_plus + n_minus))], disp_send)
    left(msg.at[pl.ds(0, 4 * hop + 1)], disp_send)

    @pl.when(c == 1)
    def _():
        left(relay_p, rel_send)
        left(relay_m, rel_send)

    left(sqs_rx.at[pl.ds(0, ntp - 1)], tp_send)
    left(spart_rx.at[pl.ds(0, ntp - 1)], tp_send)
    left(spart_half, tp_send)
    for group in range(2):
        left(sq_rx.at[group, pl.ds(0, ntp - 1)], tp_send)
        left(part_rx.at[group, pl.ds(0, ntp - 1)], tp_send)
        left(part_rx.at[group, pl.ds(0, ntp - 1), 0], tp_send)


def local(sizes, tokens, norm_gain, routes, route_weights, eg, eu, ed, sg, su, sd):
    nz, ny, nx, hop = sizes
    ntp = ny * nx
    tok_n, width = tokens.shape
    picks = routes.shape[1]
    ff = eg.shape[2]
    chunk = ff // (ntp // 2)
    slots = 4 * nz
    rows = slots // 2
    half = rows // 2
    n_plus, n_minus = nz // 2 - 1 - hop, nz // 2 - hop
    vm = pltpu.VMEM
    scratch = [
        vm((tok_n, width), BF16),
        vm((1, width), F32),
        vm((tok_n, picks), jnp.int32),
        vm((tok_n, picks), F32),
        vm((width, ff), BF16),
        vm((width, ff), BF16),
        vm((ff, width), BF16),
        vm((width, ff), BF16),
        vm((width, ff), BF16),
        vm((ff, width), BF16),
        vm((16, width), BF16),
        vm((16, picks), jnp.int32),
        vm((16, picks), F32),
        vm((16, slots), F32),
        vm((16, width), F32),
        vm((slots // 2, 2, width), BF16),
        vm((2 * n_plus, 2, 2, width), BF16),
        vm((2 * n_minus, 2, 2, width), BF16),
        vm((2, rows // 2, 2, width), BF16),
        vm((2, 1, 128), F32),
        vm((2, ntp, 1, 128), F32),
        vm((1, 128), F32),
        vm((ntp, 1, 128), F32),
        vm((2, ntp, 2, half, chunk), BF16),
        vm((2, ntp, 2, half, chunk), BF16),
        vm((ntp, 2, 8, chunk), F32),
        vm((ntp, 2, 8, chunk), F32),
        vm((2, half, chunk), BF16),
        vm((2, rows, ff), BF16),
        vm((8, chunk), BF16),
        vm((2, 8, ff), BF16),
        vm((2, rows // 2, 2, width), BF16),
        vm((slots // 2, 2, width), BF16),
        pltpu.SemaphoreType.DMA((10,)),
        pltpu.SemaphoreType.DMA,
        pltpu.SemaphoreType.DMA((2,)),
        pltpu.SemaphoreType.DMA,
        pltpu.SemaphoreType.DMA((2,)),
        pltpu.SemaphoreType.DMA,
        pltpu.SemaphoreType.DMA((3,)),
        pltpu.SemaphoreType.DMA((3,)),
        pltpu.SemaphoreType.DMA((3,)),
        pltpu.SemaphoreType.DMA,
        pltpu.SemaphoreType.DMA,
    ]
    return pl.pallas_call(
        functools.partial(kernel, sizes),
        out_shape=jax.ShapeDtypeStruct((tok_n, width), BF16),
        in_specs=[pl.BlockSpec(memory_space=pl.ANY)] * 10,
        out_specs=pl.BlockSpec(memory_space=pltpu.VMEM),
        scratch_shapes=scratch,
        compiler_params=pltpu.CompilerParams(collective_id=0, has_side_effects=True),
        name="moe_step",
    )(tokens, norm_gain.reshape(1, width), routes, route_weights, eg, eu, ed, sg, su, sd)


def on_torus(torus):
    n = torus.shape
    sizes = (n["z"], n["y"], n["x"], n["z"] // 4)
    ep, tp = ("z", "c"), ("y", "x")
    in_specs = (
        P(ep, tp),
        P(tp),
        P(ep, None),
        P(ep, None),
        P(ep, tp, None),
        P(ep, tp, None),
        P(ep, None, tp),
        P(tp, None),
        P(tp, None),
        P(None, tp),
    )
    return jax.shard_map(
        functools.partial(local, sizes),
        mesh=torus,
        in_specs=in_specs,
        out_specs=P(ep, tp),
        check_vma=False,
    )


def solution(mesh):
    return on_torus(Mesh(mesh.devices.reshape(32, 2, 4, 4), ("z", "c", "y", "x")))
```

```python
import functools

import jax
import jax.numpy as jnp
from jax import lax
from jax.experimental import pallas as pl
from jax.experimental.pallas import tpu as pltpu
from jax.sharding import Mesh
from jax.sharding import PartitionSpec as P

MESH = pl.DeviceIdType.MESH
F32 = jnp.float32
BF16 = jnp.bfloat16
DOWN_SCALE = 2.0**-40
UP_SCALE = 2.0**40


def silu(v):
    return v / (1.0 + jnp.exp(-v))


def row_of(col, width):
    rows = col.shape[0]
    eye = lax.broadcasted_iota(jnp.int32, (rows, width), 0) == lax.broadcasted_iota(
        jnp.int32, (rows, width), 1
    )
    return jnp.sum(jnp.where(eye, col, 0.0), axis=0, keepdims=True)


def col_of(row, rows, first):
    width = row.shape[1]
    eye = lax.broadcasted_iota(jnp.int32, (rows, width), 0) + first == lax.broadcasted_iota(
        jnp.int32, (rows, width), 1
    )
    return jnp.sum(jnp.where(eye, row, 0.0), axis=1, keepdims=True)


def rings(nz):
    return (0, nz // 4, nz // 2, nz)


def kernel(
    sizes,
    tok_hbm,
    gain_hbm,
    routes_hbm,
    weights_hbm,
    eg_hbm,
    eu_hbm,
    ed_hbm,
    sg_hbm,
    su_hbm,
    sd_hbm,
    out_ref,
    tok,
    gain,
    routes,
    weights,
    eg,
    eu,
    ed,
    sg,
    su,
    sd,
    tok16,
    routes16,
    weights16,
    slotw,
    shared_out,
    msg,
    relay_p,
    relay_m,
    rx,
    sq_tx,
    sq_rx,
    spart_tx,
    spart_rx,
    shid_tx,
    shid,
    hid,
    ret,
    back,
    part_tx,
    part_rx,
    hid_tx,
    load_sem,
    disp_send,
    disp_recv,
    rel_send,
    rel_recv,
    tp_send,
    sq_recv,
    part_recv,
    hid_recv,
    ret_send,
    ret_recv,
    entered,
):
    nz, ny, nx, hop = sizes
    ntp = ny * nx
    half_z = nz // 2
    ends = rings(nz)
    groups = len(ends) - 1
    close = hop // 2
    picks, tok_n = routes.shape
    width = tok.shape[1]
    total_width = float(width * ntp)
    slots = 4 * nz
    ff = eg.shape[1]
    chunk = ff // (ntp // 2)
    n_plus, n_minus = half_z - hop, half_z - 1 - hop
    least = 1 - half_z

    z, c = lax.axis_index("z"), lax.axis_index("c")
    y, x = lax.axis_index("y"), lax.axis_index("x")
    me = y * nx + x
    my_half, my_chunk = lax.rem(me, 2), me // 2

    def at(d):
        return lax.rem(z + d + 2 * nz, nz)

    def peer(i):
        j = lax.rem(me + i, ntp)
        return j, (z, c, j // nx, lax.rem(j, nx))

    barrier = pltpu.get_barrier_semaphore()

    def greet_z(i, carry):
        for core in range(2):
            for d in (close - i, i - close):
                pl.semaphore_signal(
                    barrier, inc=1, device_id=(at(d), core, y, x), device_id_type=MESH
                )
        return carry

    def greet_tp(i, carry):
        pl.semaphore_signal(barrier, inc=1, device_id=peer(i)[1], device_id_type=MESH)
        return carry

    lax.fori_loop(0, close, greet_z, 0)
    pl.semaphore_signal(barrier, inc=1, device_id=(z, 1 - c, y, x), device_id_type=MESH)
    lax.fori_loop(1, ntp, greet_tp, 0)

    loads = []
    for i, (src, dst) in enumerate(
        (
            (tok_hbm, tok),
            (routes_hbm, routes),
            (weights_hbm, weights),
            (gain_hbm, gain),
            (sg_hbm, sg),
            (su_hbm, su),
            (eg_hbm.at[0], eg),
            (eu_hbm.at[0], eu),
            (sd_hbm, sd),
            (ed_hbm.at[0], ed),
        )
    ):
        copy = pltpu.make_async_copy(src, dst, load_sem.at[i])
        copy.start()
        loads.append(copy)

    tok16[...] = jnp.zeros_like(tok16)
    routes16[...] = jnp.full_like(routes16, -1)
    weights16[...] = jnp.ones_like(weights16)
    for i in range(4):
        loads[i].wait()
    tok16[0:tok_n, :] = tok[...]
    routes16[:, 0:tok_n] = routes[...]
    weights16[:, 0:tok_n] = weights[...]
    picked, affinity = routes16[...], weights16[...]
    slot = lax.broadcasted_iota(jnp.int32, (slots, 16), 0)
    chip = slot // 4 + (z + nz + least)
    chip = jnp.where(chip >= nz, chip - nz, chip)
    chip = jnp.where(chip >= nz, chip - nz, chip)
    expert = chip * 2 + (slot // 2) % 2
    scaled = 2.5 * affinity / jnp.sum(affinity, axis=0, keepdims=True)
    named = jnp.zeros((slots, 16), F32)
    weight = jnp.zeros((slots, 16), F32)
    for k in range(picks):
        hit = picked[k : k + 1, :] == expert
        named = jnp.where(hit, 1.0, named)
        weight = jnp.where(hit, scaled[k : k + 1, :], weight)
    earlier = (
        lax.broadcasted_iota(jnp.int32, (16, 16), 0) < lax.broadcasted_iota(jnp.int32, (16, 16), 1)
    ).astype(F32)
    before = jnp.dot(named, earlier, preferred_element_type=F32)
    rank = (slot % 2).astype(F32)
    select = jnp.where(before == rank, named, 0.0)
    slot_weight = jnp.where(before == rank, weight, 0.0)
    tokens16 = tok16[...]
    outgoing = jnp.dot(select.astype(BF16), tokens16, preferred_element_type=F32).astype(BF16)
    for i in range(slots // 2):
        msg[i] = outgoing[2 * i : 2 * i + 2, :]

    with jax.named_scope("w_barrier"):
        pl.semaphore_wait(barrier, 4 * close + 1 + ntp - 1)

    def tell(sem, d, core):
        pl.semaphore_signal(sem, inc=1, device_id=(at(d), core, y, x), device_id_type=MESH)

    tell(entered.at[0], -close, c)
    tell(entered.at[1], close, c)

    def bundle(first, count, landing, target, k):
        return pltpu.make_async_remote_copy(
            src_ref=msg.at[pl.ds(2 * (first - least), 2 * count)],
            dst_ref=landing.at[:, c],
            send_sem=disp_send,
            recv_sem=rel_recv.at[k],
            device_id=(target, 1, y, x),
            device_id_type=MESH,
        )

    def ring(source):
        return source // ends[1] - source // (3 * ends[1])

    def send_near(d, core):
        pltpu.make_async_remote_copy(
            src_ref=msg.at[2 * (d - least) + core],
            dst_ref=rx.at[2 * z + c],
            send_sem=disp_send,
            recv_sem=disp_recv.at[ring(z)],
            device_id=(at(d), core, y, x),
            device_id_type=MESH,
        ).start()

    def near_plus(i, carry):
        for core in range(2):
            send_near(hop - i, core)
        return carry

    def near_minus(i, carry):
        for core in range(2):
            send_near(i - hop, core)
        return carry

    with jax.named_scope("w_plus"):
        pl.semaphore_wait(entered.at[0], 1)
    bundle(hop + 1, n_plus, relay_p, at(hop), 0).start()
    lax.fori_loop(0, hop, near_plus, 0)
    with jax.named_scope("w_minus"):
        pl.semaphore_wait(entered.at[1], 1)
    bundle(least, n_minus, relay_m, at(-hop), 1).start()

    @pl.when(c == 1)
    def _():
        tell(entered.at[2], -hop, 1)
        tell(entered.at[3], hop, 1)

    lax.fori_loop(0, hop, near_minus, 0)
    send_near(0, 1 - c)
    rx[2 * z + c] = msg[c - 2 * least]

    def to_tp(src, dst, recv):
        def one(i, carry):
            j, device = peer(i)
            pltpu.make_async_remote_copy(
                src_ref=src(j),
                dst_ref=dst,
                send_sem=tp_send,
                recv_sem=recv,
                device_id=device,
                device_id_type=MESH,
            ).start()
            return carry

        lax.fori_loop(1, ntp, one, 0)

    def waiting(src, dst, send, recv):
        return pltpu.make_async_remote_copy(
            src_ref=src,
            dst_ref=dst,
            send_sem=send,
            recv_sem=recv,
            device_id=peer(1)[1],
            device_id_type=MESH,
        )

    gains = gain[...] * DOWN_SCALE
    values = tokens16.astype(F32)
    scaled_tok = (values * gains).astype(BF16)
    sq_tx[groups] = row_of(jnp.sum(values * values, axis=1, keepdims=True), 128)
    sq_rx[groups, me] = sq_tx[groups]
    for i in (4, 5):
        loads[i].wait()
    for n, w in enumerate((sg, su)):
        part = jnp.dot(scaled_tok, w[...], preferred_element_type=F32)
        for k in range(ntp // 2):
            for h in range(2):
                spart_tx[2 * k + h, n] = part[8 * h : 8 * h + 8, k * chunk : (k + 1) * chunk]
    spart_rx[me] = spart_tx[me]

    to_tp(lambda j: sq_tx.at[groups], sq_rx.at[groups, me], sq_recv.at[groups])
    slot_weight = slot_weight.T
    for i in range(3):
        term = slot_weight.astype(BF16)
        slotw[16 * i : 16 * i + 16, :] = term
        slot_weight = slot_weight - term.astype(F32)
    to_tp(lambda j: spart_tx.at[j], spart_rx.at[me], part_recv.at[groups])

    def forward(landing, i, source, first):
        for core in range(2):
            pltpu.make_async_remote_copy(
                src_ref=landing.at[2 * i + core],
                dst_ref=rx.at[pl.ds(2 * source, 2)],
                send_sem=rel_send,
                recv_sem=disp_recv.at[ring(source)],
                device_id=(at(first + i), core, y, x),
                device_id_type=MESH,
            ).start()

    @pl.when(c == 1)
    def _():
        with jax.named_scope("w_entered"):
            pl.semaphore_wait(entered.at[2], 1)
        with jax.named_scope("w_relp"):
            waiting(relay_p, relay_p, rel_send, rel_recv.at[0]).wait_recv()

        def forward_plus(k, carry):
            forward(relay_p, n_plus - 1 - k, at(-hop), 1)
            return carry

        lax.fori_loop(0, n_plus, forward_plus, 0)
        pl.semaphore_wait(entered.at[3], 1)
        with jax.named_scope("w_relm"):
            waiting(relay_m, relay_m, rel_send, rel_recv.at[1]).wait_recv()

        def forward_minus(i, carry):
            forward(relay_m, i, at(hop), hop + least)
            return carry

        lax.fori_loop(0, n_minus, forward_minus, 0)

    def gate_up(group):
        first, last = 2 * ends[group], 2 * ends[group + 1]
        rows = 2 * (last - first)
        half = rows // 2
        mine = ring(z) == group
        with jax.named_scope(f"w_rows{group}"):
            for count, there in ((last - first - 1, mine), (last - first, jnp.logical_not(mine))):
                arrived = rx.at[pl.ds(first, count)]

                @pl.when(there)
                def _():
                    waiting(arrived, arrived, disp_send, disp_recv.at[group]).wait_recv()

        values = rx[first:last].reshape(rows, width).astype(F32)
        lhs = (values * gains).astype(BF16)
        for n, w in enumerate((eg, eu)):
            part = jnp.dot(lhs, w[...], preferred_element_type=F32).astype(BF16)
            for k in range(ntp // 2):
                for h in range(2):
                    part_tx[group][2 * k + h, n] = part[
                        half * h : half * (h + 1), k * chunk : (k + 1) * chunk
                    ]
        sq_tx[group] = row_of(jnp.sum(values * values, axis=1, keepdims=True), 128)

    def scatter(group):
        to_tp(lambda j: part_tx[group].at[j], part_rx[group].at[me], part_recv.at[group])
        to_tp(lambda j: sq_tx.at[group], sq_rx.at[group, me], sq_recv.at[group])
        sq_rx[group, me] = sq_tx[group]
        part_rx[group][me] = part_tx[group][me]

    def hidden_of(squares, parts, n):
        total = jnp.zeros((1, 128), F32)
        gate = jnp.zeros((n, chunk), F32)
        up = jnp.zeros((n, chunk), F32)
        for j in range(ntp):
            total = total + squares[j]
            gate = gate + parts[j, 0].astype(F32)
            up = up + parts[j, 1].astype(F32)
        inv = lax.rsqrt(total / total_width + 1e-06) * UP_SCALE
        inv = col_of(inv, n, my_half * n)
        return (silu(gate * inv) * (up * inv)).astype(BF16)

    def tp_wait(buf, recv):
        some = buf.at[pl.ds(0, ntp - 1)]
        waiting(some, some, tp_send, recv).wait_recv()

    columns = pl.ds(pl.multiple_of(my_chunk * chunk, chunk), chunk)

    def reduce_group(group):
        half = 2 * (ends[group + 1] - ends[group])
        base = 4 * ends[group]
        with jax.named_scope(f"w_rs{group}"):
            tp_wait(part_rx[group], part_recv.at[group])
            tp_wait(sq_rx.at[group], sq_recv.at[group])
        hid_tx[group][...] = hidden_of(sq_rx.at[group], part_rx[group], half)
        own = hid.at[pl.ds(pl.multiple_of(base + my_half * half, half), half), columns]
        to_tp(lambda j: hid_tx[group], own, hid_recv.at[group])
        own[...] = hid_tx[group][...]

    shared_blocks = part_rx[groups - 1].at[pl.ds(0, ntp - 1), 0, pl.ds(0, 8)]

    def reduce_shared():
        with jax.named_scope("w_rss"):
            tp_wait(sq_rx.at[groups], sq_recv.at[groups])
            tp_wait(spart_rx, part_recv.at[groups])
        shid_tx[...] = hidden_of(sq_rx.at[groups], spart_rx, 8)
        own = shid.at[my_half, :, columns]
        to_tp(lambda j: shid_tx, own, hid_recv.at[groups])
        own[...] = shid_tx[...]

    def down_shared():
        with jax.named_scope("w_ags"):
            waiting(shared_blocks, shared_blocks, tp_send, hid_recv.at[groups]).wait_recv()
        hidden = jnp.concatenate([shid[0], shid[1]], axis=0)
        shared_out[...] = jnp.dot(hidden, sd[...], preferred_element_type=F32)

    def give_back(source):
        place_there = 2 * lax.rem(z - source - least + nz, nz) + c
        for core in range(2):

            @pl.when(2 * source + core != 2 * z + c)
            def _():
                pltpu.make_async_remote_copy(
                    src_ref=ret.at[2 * source + core],
                    dst_ref=back.at[place_there],
                    send_sem=ret_send,
                    recv_sem=ret_recv,
                    device_id=(source, core, y, x),
                    device_id_type=MESH,
                ).start()

    def down(group):
        low, high = ends[group], ends[group + 1]
        base, rows = 4 * low, 4 * (high - low)
        blocks = part_rx[group].at[pl.ds(0, ntp - 1), 0]
        with jax.named_scope(f"w_ag{group}"):
            waiting(blocks, blocks, tp_send, hid_recv.at[group]).wait_recv()
        result = jnp.dot(hid[base : base + rows, :], ed[...], preferred_element_type=F32)
        result = result.astype(BF16)
        for i in range(rows // 2):
            ret[2 * low + i] = result[2 * i : 2 * i + 2, :]

        def one(i, carry):
            give_back(low + i)
            return carry

        lax.fori_loop(0, high - low, one, 0)

    for i in (6, 7, 8, 9):
        loads[i].wait()
    reduce_shared()
    gate_up(0)
    scatter(0)
    gate_up(1)
    scatter(1)
    gate_up(2)
    scatter(2)
    down_shared()
    reduce_group(0)
    reduce_group(1)
    down(0)
    reduce_group(2)
    down(1)
    down(2)
    back[c - 2 * least] = ret[2 * z + c]

    got = back.at[pl.ds(0, 2 * nz - 1)]
    with jax.named_scope("w_back"):
        waiting(got, got, ret_send, ret_recv).wait_recv()
    terms = jnp.dot(
        slotw[...], back[...].reshape(slots, width), preferred_element_type=F32
    )
    routed = terms[0:16, :] + (terms[16:32, :] + terms[32:48, :])
    out_ref[...] = (shared_out[...] + routed)[0:tok_n, :].astype(BF16)

    def left(ref, sem):
        waiting(ref, ref, sem, ret_recv).wait_send()

    left(got, ret_send)
    left(msg.at[pl.ds(0, 2 * (n_plus + n_minus))], disp_send)
    left(msg.at[pl.ds(0, 4 * hop + 1)], disp_send)

    @pl.when(c == 1)
    def _():
        left(relay_p, rel_send)
        left(relay_m, rel_send)

    left(spart_rx.at[pl.ds(0, ntp - 1)], tp_send)
    left(shared_blocks, tp_send)
    for group in range(groups):
        left(part_rx[group].at[pl.ds(0, ntp - 1)], tp_send)
        left(part_rx[group].at[pl.ds(0, ntp - 1), 0], tp_send)
    for group in range(groups + 1):
        left(sq_rx.at[group, pl.ds(0, ntp - 1)], tp_send)


def local(sizes, tokens, norm_gain, routes, route_weights, eg, eu, ed, sg, su, sd):
    nz, ny, nx, hop = sizes
    ntp = ny * nx
    tok_n, width = tokens.shape
    picks = routes.shape[1]
    ff = eg.shape[2]
    chunk = ff // (ntp // 2)
    slots = 4 * nz
    ends = rings(nz)
    groups = len(ends) - 1
    halves = [2 * (high - low) for low, high in zip(ends, ends[1:])]
    n_plus, n_minus = nz // 2 - hop, nz // 2 - 1 - hop
    vm, dma = pltpu.VMEM, pltpu.SemaphoreType.DMA
    scratch = [
        vm((tok_n, width), BF16),
        vm((1, width), F32),
        vm((picks, tok_n), jnp.int32),
        vm((picks, tok_n), F32),
        vm((width, ff), BF16),
        vm((width, ff), BF16),
        vm((ff, width), BF16),
        vm((width, ff), BF16),
        vm((width, ff), BF16),
        vm((ff, width), BF16),
        vm((16, width), BF16),
        vm((picks, 16), jnp.int32),
        vm((picks, 16), F32),
        vm((48, slots), BF16),
        vm((16, width), F32),
        vm((slots // 2, 2, width), BF16),
        vm((2 * n_plus, 2, 2, width), BF16),
        vm((2 * n_minus, 2, 2, width), BF16),
        vm((slots // 2, 2, width), BF16),
        vm((groups + 1, 1, 128), F32),
        vm((groups + 1, ntp, 1, 128), F32),
        vm((ntp, 2, 8, chunk), F32),
        vm((ntp, 2, 8, chunk), F32),
        vm((8, chunk), BF16),
        vm((2, 8, ff), BF16),
        vm((slots, ff), BF16),
        vm((slots // 2, 2, width), BF16),
        vm((slots // 2, 2, width), BF16),
        [vm((ntp, 2, half, chunk), BF16) for half in halves],
        [vm((ntp, 2, half, chunk), BF16) for half in halves],
        [vm((half, chunk), BF16) for half in halves],
        dma((10,)),
        dma,
        dma((groups,)),
        dma,
        dma((2,)),
        dma,
        dma((groups + 1,)),
        dma((groups + 1,)),
        dma((groups + 1,)),
        dma,
        dma,
        pltpu.SemaphoreType.REGULAR((4,)),
    ]
    return pl.pallas_call(
        functools.partial(kernel, sizes),
        out_shape=jax.ShapeDtypeStruct((tok_n, width), BF16),
        in_specs=[pl.BlockSpec(memory_space=pl.ANY)] * 10,
        out_specs=pl.BlockSpec(memory_space=pltpu.VMEM),
        scratch_shapes=scratch,
        compiler_params=pltpu.CompilerParams(collective_id=0, has_side_effects=True),
        name="moe_step",
    )(tokens, norm_gain.reshape(1, width), routes.T, route_weights.T, eg, eu, ed, sg, su, sd)


def on_torus(torus):
    n = torus.shape
    sizes = (n["z"], n["y"], n["x"], (3 * n["z"] + 14) // 16)
    ep, tp = ("z", "c"), ("y", "x")
    in_specs = (
        P(ep, tp),
        P(tp),
        P(ep, None),
        P(ep, None),
        P(ep, tp, None),
        P(ep, tp, None),
        P(ep, None, tp),
        P(tp, None),
        P(tp, None),
        P(None, tp),
    )
    return jax.shard_map(
        functools.partial(local, sizes),
        mesh=torus,
        in_specs=in_specs,
        out_specs=P(ep, tp),
        check_vma=False,
    )


def solution(mesh):
    return on_torus(Mesh(mesh.devices.reshape(32, 2, 4, 4), ("z", "c", "y", "x")))
```

```python
import functools

import jax
import jax.numpy as jnp
from jax import lax
from jax.experimental import pallas as pl
from jax.experimental.pallas import tpu as pltpu
from jax.sharding import Mesh
from jax.sharding import PartitionSpec as P

MESH = pl.DeviceIdType.MESH
F32 = jnp.float32
BF16 = jnp.bfloat16
DOWN_SCALE = 2.0**-40
UP_SCALE = 2.0**40


def silu(v):
    return v / (1.0 + jnp.exp(-v))


def row_of(col, width):
    rows = col.shape[0]
    eye = lax.broadcasted_iota(jnp.int32, (rows, width), 0) == lax.broadcasted_iota(
        jnp.int32, (rows, width), 1
    )
    return jnp.sum(jnp.where(eye, col, 0.0), axis=0, keepdims=True)


def three_terms(v):
    high = v.astype(BF16)
    rest = v - high.astype(F32)
    middle = rest.astype(BF16)
    return high, middle, (rest - middle.astype(F32)).astype(BF16)


def col_of(row, rows, first):
    width = row.shape[1]
    eye = lax.broadcasted_iota(jnp.int32, (rows, width), 0) + first == lax.broadcasted_iota(
        jnp.int32, (rows, width), 1
    )
    return jnp.sum(jnp.where(eye, row, 0.0), axis=1, keepdims=True)


def rings(nz):
    return (0, nz // 4, nz // 2, nz)


def kernel(
    sizes,
    tok_hbm,
    gain_hbm,
    routes_hbm,
    weights_hbm,
    eg_hbm,
    eu_hbm,
    ed_hbm,
    sg_hbm,
    su_hbm,
    sd_hbm,
    out_ref,
    tok,
    gain,
    routes,
    weights,
    eg,
    eu,
    ed,
    sg,
    su,
    sd,
    tok16,
    routes16,
    weights16,
    slotw,
    shared_out,
    msg,
    relay_p,
    relay_m,
    rx,
    spart_tx,
    spart_rx,
    shid_tx,
    shid,
    hid,
    ret,
    back,
    part_tx,
    part_rx,
    hid_tx,
    load_sem,
    disp_send,
    disp_recv,
    rel_send,
    rel_recv,
    tp_send,
    part_recv,
    hid_recv,
    ret_send,
    ret_recv,
    entered,
):
    nz, ny, nx, hop = sizes
    ntp = ny * nx
    half_z = nz // 2
    ends = rings(nz)
    groups = len(ends) - 1
    close = hop // 2
    picks, tok_n = routes.shape
    width = tok.shape[1]
    total_width = float(width * ntp)
    slots = 4 * nz
    ff = eg.shape[1]
    chunk = ff // (ntp // 2)
    n_plus, n_minus = half_z - hop, half_z - 1 - hop
    least = 1 - half_z

    z, c = lax.axis_index("z"), lax.axis_index("c")
    y, x = lax.axis_index("y"), lax.axis_index("x")
    me = y * nx + x
    my_half, my_chunk = lax.rem(me, 2), me // 2

    def at(d):
        return lax.rem(z + d + 2 * nz, nz)

    def peer(i):
        j = lax.rem(me + i, ntp)
        return j, (z, c, lax.div(j, nx), lax.rem(j, nx))

    barrier = pltpu.get_barrier_semaphore()

    def greet_z(i, carry):
        for core in range(2):
            for d in (close - i, i - close):
                pl.semaphore_signal(
                    barrier, inc=1, device_id=(at(d), core, y, x), device_id_type=MESH
                )
        return carry

    def in_row(i):
        return z, c, y, lax.rem(x + i, nx)

    def in_column(i):
        return z, c, lax.rem(y + i, ny), x

    lax.fori_loop(0, close, greet_z, 0)
    pl.semaphore_signal(barrier, inc=1, device_id=(z, 1 - c, y, x), device_id_type=MESH)
    for i in range(1, nx):
        pl.semaphore_signal(barrier, inc=1, device_id=in_row(i), device_id_type=MESH)
    for i in range(1, ny):
        pl.semaphore_signal(barrier, inc=1, device_id=in_column(i), device_id_type=MESH)

    loads = []
    for i, (src, dst) in enumerate(
        (
            (tok_hbm, tok),
            (routes_hbm, routes),
            (weights_hbm, weights),
            (gain_hbm, gain),
            (sg_hbm, sg),
            (su_hbm, su),
            (eg_hbm.at[0], eg),
            (eu_hbm.at[0], eu),
            (sd_hbm, sd),
            (ed_hbm.at[0], ed),
        )
    ):
        copy = pltpu.make_async_copy(src, dst, load_sem.at[i])
        copy.start()
        loads.append(copy)

    tok16[...] = jnp.zeros_like(tok16)
    routes16[...] = jnp.full_like(routes16, -1)
    weights16[...] = jnp.ones_like(weights16)
    for i in range(4):
        loads[i].wait()
    tok16[0:tok_n, :] = tok[...]
    routes16[:, 0:tok_n] = routes[...]
    weights16[:, 0:tok_n] = weights[...]
    picked, affinity = routes16[...], weights16[...]
    slot = lax.broadcasted_iota(jnp.int32, (slots, 16), 0)
    chip = slot // 4 + (z + nz + least)
    chip = jnp.where(chip >= nz, chip - nz, chip)
    chip = jnp.where(chip >= nz, chip - nz, chip)
    expert = chip * 2 + (slot // 2) % 2
    scaled = 2.5 * affinity / jnp.sum(affinity, axis=0, keepdims=True)
    named = jnp.zeros((slots, 16), F32)
    weight = jnp.zeros((slots, 16), F32)
    for k in range(picks):
        hit = picked[k : k + 1, :] == expert
        named = jnp.where(hit, 1.0, named)
        weight = jnp.where(hit, scaled[k : k + 1, :], weight)
    earlier = (
        lax.broadcasted_iota(jnp.int32, (16, 16), 0) < lax.broadcasted_iota(jnp.int32, (16, 16), 1)
    ).astype(F32)
    before = jnp.dot(named, earlier, preferred_element_type=F32)
    rank = (slot % 2).astype(F32)
    select = jnp.where(before == rank, named, 0.0)
    slot_weight = jnp.where(before == rank, weight, 0.0)
    tokens16 = tok16[...]
    outgoing = jnp.dot(select.astype(BF16), tokens16, preferred_element_type=F32).astype(BF16)
    for i in range(slots // 2):
        msg[i] = outgoing[2 * i : 2 * i + 2, :]

    with jax.named_scope("w_barrier"):
        pl.semaphore_wait(barrier, 4 * close + 1 + nx - 1 + ny - 1)

    def tell(sem, d, core):
        pl.semaphore_signal(sem, inc=1, device_id=(at(d), core, y, x), device_id_type=MESH)

    tell(entered.at[0], -close, c)
    tell(entered.at[1], close, c)

    def bundle(first, count, landing, target, k):
        return pltpu.make_async_remote_copy(
            src_ref=msg.at[pl.ds(2 * (first - least), 2 * count)],
            dst_ref=landing.at[:, c],
            send_sem=disp_send,
            recv_sem=rel_recv.at[k],
            device_id=(target, 1, y, x),
            device_id_type=MESH,
        )

    def ring(source):
        return source // ends[1] - source // (3 * ends[1])

    def send_near(d, core):
        pltpu.make_async_remote_copy(
            src_ref=msg.at[2 * (d - least) + core],
            dst_ref=rx.at[2 * z + c],
            send_sem=disp_send,
            recv_sem=disp_recv.at[ring(z)],
            device_id=(at(d), core, y, x),
            device_id_type=MESH,
        ).start()

    def near_plus(i, carry):
        for core in range(2):
            send_near(hop - i, core)
        return carry

    def near_minus(i, carry):
        for core in range(2):
            send_near(i - hop, core)
        return carry

    with jax.named_scope("w_plus"):
        pl.semaphore_wait(entered.at[0], 1)
    bundle(hop + 1, n_plus, relay_p, at(hop), 0).start()
    with jax.named_scope("w_minus"):
        pl.semaphore_wait(entered.at[1], 1)

    @pl.when(c == 1)
    def _():
        tell(entered.at[2], -hop, 1)
        tell(entered.at[3], hop, 1)

    bundle(least, n_minus, relay_m, at(-hop), 1).start()
    for i in range(1, ny):
        pl.semaphore_signal(entered.at[4], inc=1, device_id=in_column(i), device_id_type=MESH)
    lax.fori_loop(0, hop, near_plus, 0)
    lax.fori_loop(0, hop, near_minus, 0)
    send_near(0, 1 - c)
    rx[2 * z + c] = msg[c - 2 * least]

    def to_tp(src, dst, recv):
        def one(i, carry):
            j, device = peer(i)
            pltpu.make_async_remote_copy(
                src_ref=src(j),
                dst_ref=dst,
                send_sem=tp_send,
                recv_sem=recv,
                device_id=device,
                device_id_type=MESH,
            ).start()
            return carry

        lax.fori_loop(1, ntp, one, 0)

    def waiting(src, dst, send, recv):
        return pltpu.make_async_remote_copy(
            src_ref=src,
            dst_ref=dst,
            send_sem=send,
            recv_sem=recv,
            device_id=peer(1)[1],
            device_id_type=MESH,
        )

    gains = gain[...] * DOWN_SCALE
    values = tokens16.astype(F32)
    scaled_tok = (values * gains).astype(BF16)
    squares = row_of(jnp.sum(values * values, axis=1, keepdims=True), 128)
    for j in range(ntp):
        spart_tx[j, 16:24] = jnp.concatenate([squares, jnp.zeros((7, 128), F32)], axis=0)
    for i in (4, 5):
        loads[i].wait()
    for n, w in enumerate((sg, su)):
        part = jnp.dot(scaled_tok, w[...], preferred_element_type=F32)
        for k in range(ntp // 2):
            for h in range(2):
                spart_tx[2 * k + h, 8 * n : 8 * n + 8] = part[
                    8 * h : 8 * h + 8, k * chunk : (k + 1) * chunk
                ]
    spart_rx[me] = spart_tx[me]

    if ny > 1:
        pl.semaphore_wait(entered.at[4], ny - 1)
    slot_weight = slot_weight.T
    for i in range(3):
        term = slot_weight.astype(BF16)
        slotw[16 * i : 16 * i + 16, :] = term
        slot_weight = slot_weight - term.astype(F32)
    to_tp(lambda j: spart_tx.at[j], spart_rx.at[me], part_recv.at[groups])

    def forward(landing, i, source, first):
        for core in range(2):
            pltpu.make_async_remote_copy(
                src_ref=landing.at[2 * i + core],
                dst_ref=rx.at[pl.ds(2 * source, 2)],
                send_sem=rel_send,
                recv_sem=disp_recv.at[ring(source)],
                device_id=(at(first + i), core, y, x),
                device_id_type=MESH,
            ).start()

    def relay_up():
        with jax.named_scope("w_entered"):
            pl.semaphore_wait(entered.at[2], 1)
        with jax.named_scope("w_relp"):
            waiting(relay_p, relay_p, rel_send, rel_recv.at[0]).wait_recv()

        def one(k, carry):
            forward(relay_p, n_plus - 1 - k, at(-hop), 1)
            return carry

        lax.fori_loop(0, n_plus, one, 0)

    def relay_down():
        with jax.named_scope("w_entered"):
            pl.semaphore_wait(entered.at[3], 1)
        with jax.named_scope("w_relm"):
            waiting(relay_m, relay_m, rel_send, rel_recv.at[1]).wait_recv()

        def one(i, carry):
            forward(relay_m, i, at(hop), hop + least)
            return carry

        lax.fori_loop(0, n_minus, one, 0)

    @pl.when(jnp.logical_and(c == 1, z < nz - hop))
    def _():
        relay_up()
        relay_down()

    @pl.when(jnp.logical_and(c == 1, z >= nz - hop))
    def _():
        relay_down()
        relay_up()

    def gate_up(group):
        first, last = 2 * ends[group], 2 * ends[group + 1]
        rows = 2 * (last - first)
        half = rows // 2
        mine = ring(z) == group
        with jax.named_scope(f"w_rows{group}"):
            for count, there in ((last - first - 1, mine), (last - first, jnp.logical_not(mine))):
                arrived = rx.at[pl.ds(first, count)]

                @pl.when(there)
                def _():
                    waiting(arrived, arrived, disp_send, disp_recv.at[group]).wait_recv()

        values = rx[first:last].reshape(rows, width).astype(F32)
        lhs = (values * gains).astype(BF16)
        for n, w in enumerate((eg, eu)):
            part = jnp.dot(lhs, w[...], preferred_element_type=F32).astype(BF16)
            for k in range(ntp // 2):
                for h in range(2):
                    part_tx[group][2 * k + h, half * n : half * (n + 1)] = part[
                        half * h : half * (h + 1), k * chunk : (k + 1) * chunk
                    ]
        squares = row_of(jnp.sum(values * values, axis=1, keepdims=True), 128)
        terms = jnp.concatenate([*three_terms(squares), jnp.zeros((5, 128), BF16)], axis=0)
        for j in range(ntp):
            part_tx[group][j, 2 * half : 2 * half + 8] = terms

    def scatter(group):
        to_tp(lambda j: part_tx[group].at[j], part_rx[group].at[me], part_recv.at[group])
        part_rx[group][me] = part_tx[group][me]

    def hidden_of(parts, n):
        gate = jnp.zeros((n, chunk), F32)
        up = jnp.zeros((n, chunk), F32)
        total = jnp.zeros((8, 128), F32)
        for j in range(ntp):
            gate = gate + parts[j, 0:n].astype(F32)
            up = up + parts[j, n : 2 * n].astype(F32)
            total = total + parts[j, 2 * n : 2 * n + 8].astype(F32)
        total = total[0:1] + (total[1:2] + total[2:3])
        inv = lax.rsqrt(total / total_width + 1e-06) * UP_SCALE
        inv = col_of(inv, n, my_half * n)
        return (silu(gate * inv) * (up * inv)).astype(BF16)

    def tp_wait(buf, recv):
        some = buf.at[pl.ds(0, ntp - 1)]
        waiting(some, some, tp_send, recv).wait_recv()

    columns = pl.ds(pl.multiple_of(my_chunk * chunk, chunk), chunk)

    def reduce_group(group):
        half = 2 * (ends[group + 1] - ends[group])
        base = 4 * ends[group]
        with jax.named_scope(f"w_rs{group}"):
            tp_wait(part_rx[group], part_recv.at[group])
        hid_tx[group][...] = hidden_of(part_rx[group], half)
        own = hid.at[pl.ds(pl.multiple_of(base + my_half * half, half), half), columns]
        to_tp(lambda j: hid_tx[group], own, hid_recv.at[group])
        own[...] = hid_tx[group][...]

    shared_blocks = part_rx[groups - 1].at[pl.ds(0, ntp - 1), pl.ds(0, 8)]

    def reduce_shared():
        with jax.named_scope("w_rss"):
            tp_wait(spart_rx, part_recv.at[groups])
        shid_tx[...] = hidden_of(spart_rx, 8)
        own = shid.at[my_half, :, columns]
        to_tp(lambda j: shid_tx, own, hid_recv.at[groups])
        own[...] = shid_tx[...]

    def down_shared():
        with jax.named_scope("w_ags"):
            waiting(shared_blocks, shared_blocks, tp_send, hid_recv.at[groups]).wait_recv()
        hidden = jnp.concatenate([shid[0], shid[1]], axis=0)
        shared_out[...] = jnp.dot(hidden, sd[...], preferred_element_type=F32)

    def give_back(source):
        place_there = 2 * lax.rem(z - source - least + nz, nz) + c
        for core in range(2):

            @pl.when(2 * source + core != 2 * z + c)
            def _():
                pltpu.make_async_remote_copy(
                    src_ref=ret.at[2 * source + core],
                    dst_ref=back.at[place_there],
                    send_sem=ret_send,
                    recv_sem=ret_recv,
                    device_id=(source, core, y, x),
                    device_id_type=MESH,
                ).start()

    def down(group):
        low, high = ends[group], ends[group + 1]
        base, rows = 4 * low, 4 * (high - low)
        blocks = part_rx[group].at[pl.ds(0, ntp - 1), pl.ds(0, rows // 2)]
        with jax.named_scope(f"w_ag{group}"):
            waiting(blocks, blocks, tp_send, hid_recv.at[group]).wait_recv()
        result = jnp.dot(hid[base : base + rows, :], ed[...], preferred_element_type=F32)
        result = result.astype(BF16)
        for i in range(rows // 2):
            ret[2 * low + i] = result[2 * i : 2 * i + 2, :]

        def one(i, carry):
            give_back(low + i)
            return carry

        lax.fori_loop(0, high - low, one, 0)

    for i in (6, 7, 8, 9):
        loads[i].wait()
    reduce_shared()
    gate_up(0)
    scatter(0)
    gate_up(1)
    gate_up(2)
    down_shared()
    reduce_group(0)
    scatter(1)
    down(0)
    scatter(2)
    reduce_group(1)
    down(1)
    reduce_group(2)
    down(2)
    back[c - 2 * least] = ret[2 * z + c]

    got = back.at[pl.ds(0, 2 * nz - 1)]
    with jax.named_scope("w_back"):
        waiting(got, got, ret_send, ret_recv).wait_recv()
    terms = jnp.dot(
        slotw[...], back[...].reshape(slots, width), preferred_element_type=F32
    )
    routed = terms[0:16, :] + (terms[16:32, :] + terms[32:48, :])
    out_ref[...] = (shared_out[...] + routed)[0:tok_n, :].astype(BF16)

    def left(ref, sem):
        waiting(ref, ref, sem, ret_recv).wait_send()

    left(got, ret_send)
    left(msg.at[pl.ds(0, 2 * (n_plus + n_minus))], disp_send)
    left(msg.at[pl.ds(0, 4 * hop + 1)], disp_send)

    @pl.when(c == 1)
    def _():
        left(relay_p, rel_send)
        left(relay_m, rel_send)

    left(spart_rx.at[pl.ds(0, ntp - 1)], tp_send)
    left(shared_blocks, tp_send)
    for group in range(groups):
        left(part_rx[group].at[pl.ds(0, ntp - 1)], tp_send)
        half = 2 * (ends[group + 1] - ends[group])
        left(part_rx[group].at[pl.ds(0, ntp - 1), pl.ds(0, half)], tp_send)


def local(sizes, tokens, norm_gain, routes, route_weights, eg, eu, ed, sg, su, sd):
    nz, ny, nx, hop = sizes
    ntp = ny * nx
    tok_n, width = tokens.shape
    picks = routes.shape[1]
    ff = eg.shape[2]
    chunk = ff // (ntp // 2)
    slots = 4 * nz
    ends = rings(nz)
    groups = len(ends) - 1
    halves = [2 * (high - low) for low, high in zip(ends, ends[1:])]
    n_plus, n_minus = nz // 2 - hop, nz // 2 - 1 - hop
    vm, dma = pltpu.VMEM, pltpu.SemaphoreType.DMA
    scratch = [
        vm((tok_n, width), BF16),
        vm((1, width), F32),
        vm((picks, tok_n), jnp.int32),
        vm((picks, tok_n), F32),
        vm((width, ff), BF16),
        vm((width, ff), BF16),
        vm((ff, width), BF16),
        vm((width, ff), BF16),
        vm((width, ff), BF16),
        vm((ff, width), BF16),
        vm((16, width), BF16),
        vm((picks, 16), jnp.int32),
        vm((picks, 16), F32),
        vm((48, slots), BF16),
        vm((16, width), F32),
        vm((slots // 2, 2, width), BF16),
        vm((2 * n_plus, 2, 2, width), BF16),
        vm((2 * n_minus, 2, 2, width), BF16),
        vm((slots // 2, 2, width), BF16),
        vm((ntp, 24, chunk), F32),
        vm((ntp, 24, chunk), F32),
        vm((8, chunk), BF16),
        vm((2, 8, ff), BF16),
        vm((slots, ff), BF16),
        vm((slots // 2, 2, width), BF16),
        vm((slots // 2, 2, width), BF16),
        [vm((ntp, 2 * half + 8, chunk), BF16) for half in halves],
        [vm((ntp, 2 * half + 8, chunk), BF16) for half in halves],
        [vm((half, chunk), BF16) for half in halves],
        dma((10,)),
        dma,
        dma((groups,)),
        dma,
        dma((2,)),
        dma,
        dma((groups + 1,)),
        dma((groups + 1,)),
        dma,
        dma,
        pltpu.SemaphoreType.REGULAR((5,)),
    ]
    return pl.pallas_call(
        functools.partial(kernel, sizes),
        out_shape=jax.ShapeDtypeStruct((tok_n, width), BF16),
        in_specs=[pl.BlockSpec(memory_space=pl.ANY)] * 10,
        out_specs=pl.BlockSpec(memory_space=pltpu.VMEM),
        scratch_shapes=scratch,
        compiler_params=pltpu.CompilerParams(collective_id=0, has_side_effects=True),
        name="moe_step",
    )(tokens, norm_gain.reshape(1, width), routes.T, route_weights.T, eg, eu, ed, sg, su, sd)


def on_torus(torus):
    n = torus.shape
    sizes = (n["z"], n["y"], n["x"], (3 * n["z"] + 14) // 16)
    ep, tp = ("z", "c"), ("y", "x")
    in_specs = (
        P(ep, tp),
        P(tp),
        P(ep, None),
        P(ep, None),
        P(ep, tp, None),
        P(ep, tp, None),
        P(ep, None, tp),
        P(tp, None),
        P(tp, None),
        P(None, tp),
    )
    return jax.shard_map(
        functools.partial(local, sizes),
        mesh=torus,
        in_specs=in_specs,
        out_specs=P(ep, tp),
        check_vma=False,
    )


def solution(mesh):
    return on_torus(Mesh(mesh.devices.reshape(32, 2, 4, 4), ("z", "c", "y", "x")))
```

```python
import functools

import jax
import jax.numpy as jnp
from jax import lax
from jax.experimental import pallas as pl
from jax.experimental.pallas import tpu as pltpu
from jax.sharding import Mesh
from jax.sharding import PartitionSpec as P

MESH = pl.DeviceIdType.MESH
F32 = jnp.float32
BF16 = jnp.bfloat16
DOWN_SCALE = 2.0**-40
UP_SCALE = 2.0**40


def silu(v):
    return v / (1.0 + jnp.exp(-v))


def row_of(col, width):
    rows = col.shape[0]
    eye = lax.broadcasted_iota(jnp.int32, (rows, width), 0) == lax.broadcasted_iota(
        jnp.int32, (rows, width), 1
    )
    return jnp.sum(jnp.where(eye, col, 0.0), axis=0, keepdims=True)


def three_terms(v):
    high = v.astype(BF16)
    rest = v - high.astype(F32)
    middle = rest.astype(BF16)
    return high, middle, (rest - middle.astype(F32)).astype(BF16)


def col_of(row, rows, first):
    width = row.shape[1]
    eye = lax.broadcasted_iota(jnp.int32, (rows, width), 0) + first == lax.broadcasted_iota(
        jnp.int32, (rows, width), 1
    )
    return jnp.sum(jnp.where(eye, row, 0.0), axis=1, keepdims=True)


def rings(nz):
    return (0, nz // 4, nz // 2, nz)


def kernel(
    sizes,
    tok_hbm,
    gain_hbm,
    routes_hbm,
    weights_hbm,
    eg_hbm,
    eu_hbm,
    ed_hbm,
    sg_hbm,
    su_hbm,
    sd_hbm,
    out_ref,
    tok,
    gain,
    routes,
    weights,
    eg,
    eu,
    ed,
    sg,
    su,
    sd,
    tok16,
    routes16,
    weights16,
    slotw,
    shared_out,
    msg,
    relay_p,
    relay_m,
    rx,
    spart_tx,
    spart_rx,
    shid_tx,
    shid,
    hid,
    ret,
    back,
    part_tx,
    part_rx,
    hid_tx,
    load_sem,
    disp_send,
    disp_recv,
    rel_send,
    rel_recv,
    tp_send,
    part_recv,
    hid_recv,
    ret_send,
    ret_recv,
    entered,
):
    nz, ny, nx, hop = sizes
    ntp = ny * nx
    half_z = nz // 2
    ends = rings(nz)
    groups = len(ends) - 1
    close = hop // 2
    picks, tok_n = routes.shape
    width = tok.shape[1]
    total_width = float(width * ntp)
    slots = 4 * nz
    ff = eg.shape[1]
    chunk = ff // (ntp // 2)
    n_plus, n_minus = half_z - hop, half_z - 1 - hop
    least = 1 - half_z

    z, c = lax.axis_index("z"), lax.axis_index("c")
    y, x = lax.axis_index("y"), lax.axis_index("x")
    me = y * nx + x
    my_half, my_chunk = lax.rem(me, 2), me // 2

    def at(d):
        return lax.rem(z + d + 2 * nz, nz)

    def peer(i):
        j = lax.rem(me + i, ntp)
        return j, (z, c, lax.div(j, nx), lax.rem(j, nx))

    barrier = pltpu.get_barrier_semaphore()

    def greet_z(i, carry):
        for core in range(2):
            for d in (close - i, i - close):
                pl.semaphore_signal(
                    barrier, inc=1, device_id=(at(d), core, y, x), device_id_type=MESH
                )
        return carry

    def in_row(i):
        return z, c, y, lax.rem(x + i, nx)

    def in_column(i):
        return z, c, lax.rem(y + i, ny), x

    lax.fori_loop(0, close, greet_z, 0)
    pl.semaphore_signal(barrier, inc=1, device_id=(z, 1 - c, y, x), device_id_type=MESH)
    for i in range(1, nx):
        pl.semaphore_signal(barrier, inc=1, device_id=in_row(i), device_id_type=MESH)
    for i in range(1, ny):
        pl.semaphore_signal(barrier, inc=1, device_id=in_column(i), device_id_type=MESH)

    loads = []
    for i, (src, dst) in enumerate(
        (
            (tok_hbm, tok),
            (routes_hbm, routes),
            (weights_hbm, weights),
            (gain_hbm, gain),
            (sg_hbm, sg),
            (su_hbm, su),
            (eg_hbm.at[0], eg),
            (eu_hbm.at[0], eu),
            (sd_hbm, sd),
            (ed_hbm.at[0], ed),
        )
    ):
        copy = pltpu.make_async_copy(src, dst, load_sem.at[i])
        copy.start()
        loads.append(copy)

    tok16[...] = jnp.zeros_like(tok16)
    routes16[...] = jnp.full_like(routes16, -1)
    weights16[...] = jnp.ones_like(weights16)
    for i in range(4):
        loads[i].wait()
    tok16[0:tok_n, :] = tok[...]
    routes16[:, 0:tok_n] = routes[...]
    weights16[:, 0:tok_n] = weights[...]
    picked, affinity = routes16[...], weights16[...]
    slot = lax.broadcasted_iota(jnp.int32, (slots, 16), 0)
    chip = slot // 4 + (z + nz + least)
    chip = jnp.where(chip >= nz, chip - nz, chip)
    chip = jnp.where(chip >= nz, chip - nz, chip)
    expert = chip * 2 + (slot // 2) % 2
    scaled = 2.5 * affinity / jnp.sum(affinity, axis=0, keepdims=True)
    named = jnp.zeros((slots, 16), F32)
    weight = jnp.zeros((slots, 16), F32)
    for k in range(picks):
        hit = picked[k : k + 1, :] == expert
        named = jnp.where(hit, 1.0, named)
        weight = jnp.where(hit, scaled[k : k + 1, :], weight)
    earlier = (
        lax.broadcasted_iota(jnp.int32, (16, 16), 0) < lax.broadcasted_iota(jnp.int32, (16, 16), 1)
    ).astype(F32)
    before = jnp.dot(named, earlier, preferred_element_type=F32)
    rank = (slot % 2).astype(F32)
    select = jnp.where(before == rank, named, 0.0)
    slot_weight = jnp.where(before == rank, weight, 0.0)
    tokens16 = tok16[...]
    outgoing = jnp.dot(select.astype(BF16), tokens16, preferred_element_type=F32).astype(BF16)
    for i in range(slots // 2):
        msg[i] = outgoing[2 * i : 2 * i + 2, :]

    with jax.named_scope("w_barrier"):
        pl.semaphore_wait(barrier, 4 * close + 1 + nx - 1 + ny - 1)

    def tell(sem, d, core):
        pl.semaphore_signal(sem, inc=1, device_id=(at(d), core, y, x), device_id_type=MESH)

    tell(entered.at[0], -close, c)
    tell(entered.at[1], close, c)

    def bundle(first, count, landing, target, k):
        return pltpu.make_async_remote_copy(
            src_ref=msg.at[pl.ds(2 * (first - least), 2 * count)],
            dst_ref=landing.at[:, c],
            send_sem=disp_send,
            recv_sem=rel_recv.at[k],
            device_id=(target, 1, y, x),
            device_id_type=MESH,
        )

    def ring(source):
        return source // ends[1] - source // (3 * ends[1])

    def send_near(d, core):
        pltpu.make_async_remote_copy(
            src_ref=msg.at[2 * (d - least) + core],
            dst_ref=rx.at[2 * z + c],
            send_sem=disp_send,
            recv_sem=disp_recv.at[ring(z)],
            device_id=(at(d), core, y, x),
            device_id_type=MESH,
        ).start()

    def near_plus(i, carry):
        for core in range(2):
            send_near(hop - i, core)
        return carry

    def near_minus(i, carry):
        for core in range(2):
            send_near(i - hop, core)
        return carry

    with jax.named_scope("w_plus"):
        pl.semaphore_wait(entered.at[0], 1)
    bundle(hop + 1, n_plus, relay_p, at(hop), 0).start()
    with jax.named_scope("w_minus"):
        pl.semaphore_wait(entered.at[1], 1)

    @pl.when(c == 1)
    def _():
        tell(entered.at[2], -hop, 1)
        tell(entered.at[3], hop, 1)

    bundle(least, n_minus, relay_m, at(-hop), 1).start()
    for i in range(1, ny):
        pl.semaphore_signal(entered.at[4], inc=1, device_id=in_column(i), device_id_type=MESH)
    lax.fori_loop(0, hop, near_plus, 0)
    lax.fori_loop(0, hop, near_minus, 0)
    send_near(0, 1 - c)
    rx[2 * z + c] = msg[c - 2 * least]

    def to_tp(src, dst, recv):
        def one(i, carry):
            j, device = peer(i)
            pltpu.make_async_remote_copy(
                src_ref=src(j),
                dst_ref=dst,
                send_sem=tp_send,
                recv_sem=recv,
                device_id=device,
                device_id_type=MESH,
            ).start()
            return carry

        lax.fori_loop(1, ntp, one, 0)

    def waiting(src, dst, send, recv):
        return pltpu.make_async_remote_copy(
            src_ref=src,
            dst_ref=dst,
            send_sem=send,
            recv_sem=recv,
            device_id=peer(1)[1],
            device_id_type=MESH,
        )

    gains = gain[...] * DOWN_SCALE
    values = tokens16.astype(F32)
    scaled_tok = (values * gains).astype(BF16)
    squares = row_of(jnp.sum(values * values, axis=1, keepdims=True), 128)
    for j in range(ntp):
        spart_tx[j, 16:24] = jnp.concatenate([squares, jnp.zeros((7, 128), F32)], axis=0)
    for i in (4, 5):
        loads[i].wait()
    for n, w in enumerate((sg, su)):
        part = jnp.dot(scaled_tok, w[...], preferred_element_type=F32)
        for k in range(ntp // 2):
            for h in range(2):
                spart_tx[2 * k + h, 8 * n : 8 * n + 8] = part[
                    8 * h : 8 * h + 8, k * chunk : (k + 1) * chunk
                ]
    spart_rx[me] = spart_tx[me]

    if ny > 1:
        pl.semaphore_wait(entered.at[4], ny - 1)
    slot_weight = slot_weight.T
    for i in range(3):
        term = slot_weight.astype(BF16)
        slotw[16 * i : 16 * i + 16, :] = term
        slot_weight = slot_weight - term.astype(F32)
    to_tp(lambda j: spart_tx.at[j], spart_rx.at[me], part_recv.at[groups])

    def forward(landing, i, source, first):
        for core in range(2):
            pltpu.make_async_remote_copy(
                src_ref=landing.at[2 * i + core],
                dst_ref=rx.at[pl.ds(2 * source, 2)],
                send_sem=rel_send,
                recv_sem=disp_recv.at[ring(source)],
                device_id=(at(first + i), core, y, x),
                device_id_type=MESH,
            ).start()

    def relay_up():
        with jax.named_scope("w_entered"):
            pl.semaphore_wait(entered.at[2], 1)
        with jax.named_scope("w_relp"):
            waiting(relay_p, relay_p, rel_send, rel_recv.at[0]).wait_recv()

        def one(k, carry):
            forward(relay_p, n_plus - 1 - k, at(-hop), 1)
            return carry

        lax.fori_loop(0, n_plus, one, 0)

    def relay_down():
        with jax.named_scope("w_entered"):
            pl.semaphore_wait(entered.at[3], 1)
        with jax.named_scope("w_relm"):
            waiting(relay_m, relay_m, rel_send, rel_recv.at[1]).wait_recv()

        def one(i, carry):
            forward(relay_m, i, at(hop), hop + least)
            return carry

        lax.fori_loop(0, n_minus, one, 0)

    @pl.when(jnp.logical_and(c == 1, z < nz - hop))
    def _():
        relay_up()
        relay_down()

    @pl.when(jnp.logical_and(c == 1, z >= nz - hop))
    def _():
        relay_down()
        relay_up()

    def gate_up(group):
        first, last = 2 * ends[group], 2 * ends[group + 1]
        rows = 2 * (last - first)
        half = rows // 2
        mine = ring(z) == group
        with jax.named_scope(f"w_rows{group}"):
            for count, there in ((last - first - 1, mine), (last - first, jnp.logical_not(mine))):
                arrived = rx.at[pl.ds(first, count)]

                @pl.when(there)
                def _():
                    waiting(arrived, arrived, disp_send, disp_recv.at[group]).wait_recv()

        values = rx[first:last].reshape(rows, width).astype(F32)
        lhs = (values * gains).astype(BF16)
        for n, w in enumerate((eg, eu)):
            part = jnp.dot(lhs, w[...], preferred_element_type=F32).astype(BF16)
            for k in range(ntp // 2):
                for h in range(2):
                    part_tx[group][2 * k + h, half * n : half * (n + 1)] = part[
                        half * h : half * (h + 1), k * chunk : (k + 1) * chunk
                    ]
        squares = row_of(jnp.sum(values * values, axis=1, keepdims=True), 128)
        terms = jnp.concatenate([*three_terms(squares), jnp.zeros((5, 128), BF16)], axis=0)
        for j in range(ntp):
            part_tx[group][j, 2 * half : 2 * half + 8] = terms

    def scatter(group):
        to_tp(lambda j: part_tx[group].at[j], part_rx[group].at[me], part_recv.at[group])
        part_rx[group][me] = part_tx[group][me]

    def hidden_of(parts, n):
        gate = jnp.zeros((n, chunk), F32)
        up = jnp.zeros((n, chunk), F32)
        total = jnp.zeros((8, 128), F32)
        for j in range(ntp):
            gate = gate + parts[j, 0:n].astype(F32)
            up = up + parts[j, n : 2 * n].astype(F32)
            total = total + parts[j, 2 * n : 2 * n + 8].astype(F32)
        total = total[0:1] + (total[1:2] + total[2:3])
        inv = lax.rsqrt(total / total_width + 1e-06) * UP_SCALE
        inv = col_of(inv, n, my_half * n)
        return (silu(gate * inv) * (up * inv)).astype(BF16)

    def tp_wait(buf, recv):
        some = buf.at[pl.ds(0, ntp - 1)]
        waiting(some, some, tp_send, recv).wait_recv()

    columns = pl.ds(pl.multiple_of(my_chunk * chunk, chunk), chunk)

    def reduce_group(group):
        half = 2 * (ends[group + 1] - ends[group])
        base = 4 * ends[group]
        with jax.named_scope(f"w_rs{group}"):
            tp_wait(part_rx[group], part_recv.at[group])
        hid_tx[group][...] = hidden_of(part_rx[group], half)
        own = hid.at[pl.ds(pl.multiple_of(base + my_half * half, half), half), columns]
        to_tp(lambda j: hid_tx[group], own, hid_recv.at[group])
        own[...] = hid_tx[group][...]

    shared_blocks = part_rx[groups - 1].at[pl.ds(0, ntp - 1), pl.ds(0, 8)]

    def reduce_shared():
        with jax.named_scope("w_rss"):
            tp_wait(spart_rx, part_recv.at[groups])
        shid_tx[...] = hidden_of(spart_rx, 8)
        own = shid.at[my_half, :, columns]
        to_tp(lambda j: shid_tx, own, hid_recv.at[groups])
        own[...] = shid_tx[...]

    def down_shared():
        with jax.named_scope("w_ags"):
            waiting(shared_blocks, shared_blocks, tp_send, hid_recv.at[groups]).wait_recv()
        hidden = jnp.concatenate([shid[0], shid[1]], axis=0)
        shared_out[...] = jnp.dot(hidden, sd[...], preferred_element_type=F32)

    def give_back(source):
        place_there = 2 * lax.rem(z - source - least + nz, nz) + c
        for core in range(2):

            @pl.when(2 * source + core != 2 * z + c)
            def _():
                pltpu.make_async_remote_copy(
                    src_ref=ret.at[2 * source + core],
                    dst_ref=back.at[place_there],
                    send_sem=ret_send,
                    recv_sem=ret_recv,
                    device_id=(source, core, y, x),
                    device_id_type=MESH,
                ).start()

    def down(group):
        low, high = ends[group], ends[group + 1]
        base, rows = 4 * low, 4 * (high - low)
        blocks = part_rx[group].at[pl.ds(0, ntp - 1), pl.ds(0, rows // 2)]
        with jax.named_scope(f"w_ag{group}"):
            waiting(blocks, blocks, tp_send, hid_recv.at[group]).wait_recv()
        result = jnp.dot(hid[base : base + rows, :], ed[...], preferred_element_type=F32)
        result = result.astype(BF16)
        for i in range(rows // 2):
            ret[2 * low + i] = result[2 * i : 2 * i + 2, :]

        def one(i, carry):
            give_back(low + i)
            return carry

        lax.fori_loop(0, high - low, one, 0)

    for i in (6, 7, 8, 9):
        loads[i].wait()
    reduce_shared()
    gate_up(0)
    scatter(0)
    gate_up(1)
    gate_up(2)
    down_shared()
    reduce_group(0)
    scatter(1)
    down(0)
    scatter(2)
    reduce_group(1)
    down(1)
    reduce_group(2)
    down(2)
    back[c - 2 * least] = ret[2 * z + c]

    got = back.at[pl.ds(0, 2 * nz - 1)]
    with jax.named_scope("w_back"):
        waiting(got, got, ret_send, ret_recv).wait_recv()
    terms = jnp.dot(
        slotw[...], back[...].reshape(slots, width), preferred_element_type=F32
    )
    routed = terms[0:16, :] + (terms[16:32, :] + terms[32:48, :])
    out_ref[...] = (shared_out[...] + routed)[0:tok_n, :].astype(BF16)

    def left(ref, sem):
        waiting(ref, ref, sem, ret_recv).wait_send()

    left(got, ret_send)
    left(msg.at[pl.ds(0, 2 * (n_plus + n_minus))], disp_send)
    left(msg.at[pl.ds(0, 4 * hop + 1)], disp_send)

    @pl.when(c == 1)
    def _():
        left(relay_p, rel_send)
        left(relay_m, rel_send)

    left(spart_rx.at[pl.ds(0, ntp - 1)], tp_send)
    left(shared_blocks, tp_send)
    for group in range(groups):
        left(part_rx[group].at[pl.ds(0, ntp - 1)], tp_send)
        half = 2 * (ends[group + 1] - ends[group])
        left(part_rx[group].at[pl.ds(0, ntp - 1), pl.ds(0, half)], tp_send)


def local(sizes, tokens, norm_gain, routes, route_weights, eg, eu, ed, sg, su, sd):
    nz, ny, nx, hop = sizes
    ntp = ny * nx
    tok_n, width = tokens.shape
    picks = routes.shape[1]
    ff = eg.shape[2]
    chunk = ff // (ntp // 2)
    slots = 4 * nz
    ends = rings(nz)
    groups = len(ends) - 1
    halves = [2 * (high - low) for low, high in zip(ends, ends[1:])]
    n_plus, n_minus = nz // 2 - hop, nz // 2 - 1 - hop
    vm, dma = pltpu.VMEM, pltpu.SemaphoreType.DMA
    scratch = [
        vm((tok_n, width), BF16),
        vm((1, width), F32),
        vm((picks, tok_n), jnp.int32),
        vm((picks, tok_n), F32),
        vm((width, ff), BF16),
        vm((width, ff), BF16),
        vm((ff, width), BF16),
        vm((width, ff), BF16),
        vm((width, ff), BF16),
        vm((ff, width), BF16),
        vm((16, width), BF16),
        vm((picks, 16), jnp.int32),
        vm((picks, 16), F32),
        vm((48, slots), BF16),
        vm((16, width), F32),
        vm((slots // 2, 2, width), BF16),
        vm((2 * n_plus, 2, 2, width), BF16),
        vm((2 * n_minus, 2, 2, width), BF16),
        vm((slots // 2, 2, width), BF16),
        vm((ntp, 24, chunk), F32),
        vm((ntp, 24, chunk), F32),
        vm((8, chunk), BF16),
        vm((2, 8, ff), BF16),
        vm((slots, ff), BF16),
        vm((slots // 2, 2, width), BF16),
        vm((slots // 2, 2, width), BF16),
        [vm((ntp, 2 * half + 8, chunk), BF16) for half in halves],
        [vm((ntp, 2 * half + 8, chunk), BF16) for half in halves],
        [vm((half, chunk), BF16) for half in halves],
        dma((10,)),
        dma,
        dma((groups,)),
        dma,
        dma((2,)),
        dma,
        dma((groups + 1,)),
        dma((groups + 1,)),
        dma,
        dma,
        pltpu.SemaphoreType.REGULAR((5,)),
    ]
    def held(a):
        return pltpu.with_memory_space_constraint(a, pltpu.HBM)

    return pl.pallas_call(
        functools.partial(kernel, sizes),
        out_shape=jax.ShapeDtypeStruct((tok_n, width), BF16),
        in_specs=[pl.BlockSpec(memory_space=pl.ANY)] * 10,
        out_specs=pl.BlockSpec(memory_space=pltpu.VMEM),
        scratch_shapes=scratch,
        compiler_params=pltpu.CompilerParams(collective_id=0, has_side_effects=True, vmem_limit_bytes=40 << 20),
        name="moe_step",
    )(*map(held, (tokens, norm_gain.reshape(1, width), routes.T, route_weights.T, eg, eu, ed, sg, su, sd)))


def on_torus(torus):
    n = torus.shape
    sizes = (n["z"], n["y"], n["x"], (3 * n["z"] + 14) // 16)
    ep, tp = ("z", "c"), ("y", "x")
    in_specs = (
        P(ep, tp),
        P(tp),
        P(ep, None),
        P(ep, None),
        P(ep, tp, None),
        P(ep, tp, None),
        P(ep, None, tp),
        P(tp, None),
        P(tp, None),
        P(None, tp),
    )
    return jax.shard_map(
        functools.partial(local, sizes),
        mesh=torus,
        in_specs=in_specs,
        out_specs=P(ep, tp),
        check_vma=False,
    )


def solution(mesh):
    return on_torus(Mesh(mesh.devices.reshape(32, 2, 4, 4), ("z", "c", "y", "x")))
```

```python
import functools

import jax
import jax.numpy as jnp
from jax import lax
from jax.experimental import pallas as pl
from jax.experimental.pallas import tpu as pltpu
from jax.sharding import Mesh
from jax.sharding import PartitionSpec as P

MESH = pl.DeviceIdType.MESH
F32 = jnp.float32
BF16 = jnp.bfloat16
DOWN_SCALE = 2.0**-40
UP_SCALE = 2.0**40


def silu(v):
    return v / (1.0 + jnp.exp(-v))


def row_of(col, width):
    rows = col.shape[0]
    eye = lax.broadcasted_iota(jnp.int32, (rows, width), 0) == lax.broadcasted_iota(
        jnp.int32, (rows, width), 1
    )
    return jnp.sum(jnp.where(eye, col, 0.0), axis=0, keepdims=True)


def three_terms(v):
    high = v.astype(BF16)
    rest = v - high.astype(F32)
    middle = rest.astype(BF16)
    return high, middle, (rest - middle.astype(F32)).astype(BF16)


def col_of(row, rows, first):
    width = row.shape[1]
    eye = lax.broadcasted_iota(jnp.int32, (rows, width), 0) + first == lax.broadcasted_iota(
        jnp.int32, (rows, width), 1
    )
    return jnp.sum(jnp.where(eye, row, 0.0), axis=1, keepdims=True)


def rings(nz):
    return (0, nz // 8, 3 * nz // 8, nz)


def kernel(
    sizes,
    tok_hbm,
    gain_hbm,
    routes_hbm,
    weights_hbm,
    eg_hbm,
    eu_hbm,
    ed_hbm,
    sg_hbm,
    su_hbm,
    sd_hbm,
    out_ref,
    tok,
    gain,
    routes,
    weights,
    eg,
    eu,
    ed,
    sg,
    su,
    sd,
    tok16,
    routes16,
    weights16,
    slotw,
    shared_out,
    msg,
    relay_p,
    relay_m,
    rx,
    spart_tx,
    spart_rx,
    shid_tx,
    shid,
    hid,
    ret,
    back,
    part_tx,
    part_rx,
    hid_tx,
    load_sem,
    disp_send,
    disp_recv,
    rel_send,
    rel_recv,
    tp_send,
    part_recv,
    hid_recv,
    ret_send,
    ret_recv,
    entered,
):
    nz, ny, nx, hop = sizes
    ntp = ny * nx
    half_z = nz // 2
    ends = rings(nz)
    groups = len(ends) - 1
    close = hop // 2
    picks, tok_n = routes.shape
    width = tok.shape[1]
    total_width = float(width * ntp)
    slots = 4 * nz
    ff = eg.shape[1]
    chunk = ff // (ntp // 2)
    n_plus, n_minus = half_z - hop, half_z - 1 - hop
    least = 1 - half_z

    z, c = lax.axis_index("z"), lax.axis_index("c")
    y, x = lax.axis_index("y"), lax.axis_index("x")
    me = y * nx + x
    my_half, my_chunk = lax.rem(me, 2), me // 2

    def at(d):
        return lax.rem(z + d + 2 * nz, nz)

    def peer(i):
        j = lax.rem(me + i, ntp)
        return j, (z, c, lax.div(j, nx), lax.rem(j, nx))

    barrier = pltpu.get_barrier_semaphore()

    def greet_z(i, carry):
        for core in range(2):
            for d in (close - i, i - close):
                pl.semaphore_signal(
                    barrier, inc=1, device_id=(at(d), core, y, x), device_id_type=MESH
                )
        return carry

    def in_row(i):
        return z, c, y, lax.rem(x + i, nx)

    def in_column(i):
        return z, c, lax.rem(y + i, ny), x

    lax.fori_loop(0, close, greet_z, 0)
    pl.semaphore_signal(barrier, inc=1, device_id=(z, 1 - c, y, x), device_id_type=MESH)
    for i in range(1, nx):
        pl.semaphore_signal(barrier, inc=1, device_id=in_row(i), device_id_type=MESH)
    for i in range(1, ny):
        pl.semaphore_signal(barrier, inc=1, device_id=in_column(i), device_id_type=MESH)

    loads = []
    for i, (src, dst) in enumerate(
        (
            (tok_hbm, tok),
            (routes_hbm, routes),
            (weights_hbm, weights),
            (gain_hbm, gain),
            (sg_hbm, sg),
            (su_hbm, su),
            (eg_hbm.at[0], eg),
            (eu_hbm.at[0], eu),
            (sd_hbm, sd),
            (ed_hbm.at[0], ed),
        )
    ):
        copy = pltpu.make_async_copy(src, dst, load_sem.at[i])
        copy.start()
        loads.append(copy)

    tok16[...] = jnp.zeros_like(tok16)
    routes16[...] = jnp.full_like(routes16, -1)
    weights16[...] = jnp.ones_like(weights16)
    for i in range(4):
        loads[i].wait()
    tok16[0:tok_n, :] = tok[...]
    routes16[:, 0:tok_n] = routes[...]
    weights16[:, 0:tok_n] = weights[...]
    picked, affinity = routes16[...], weights16[...]
    slot = lax.broadcasted_iota(jnp.int32, (slots, 16), 0)
    chip = slot // 4 + (z + nz + least)
    chip = jnp.where(chip >= nz, chip - nz, chip)
    chip = jnp.where(chip >= nz, chip - nz, chip)
    expert = chip * 2 + (slot // 2) % 2
    scaled = 2.5 * affinity / jnp.sum(affinity, axis=0, keepdims=True)
    named = jnp.zeros((slots, 16), F32)
    weight = jnp.zeros((slots, 16), F32)
    for k in range(picks):
        hit = picked[k : k + 1, :] == expert
        named = jnp.where(hit, 1.0, named)
        weight = jnp.where(hit, scaled[k : k + 1, :], weight)
    earlier = (
        lax.broadcasted_iota(jnp.int32, (16, 16), 0) < lax.broadcasted_iota(jnp.int32, (16, 16), 1)
    ).astype(F32)
    before = jnp.dot(named, earlier, preferred_element_type=F32)
    rank = (slot % 2).astype(F32)
    select = jnp.where(before == rank, named, 0.0)
    slot_weight = jnp.where(before == rank, weight, 0.0)
    tokens16 = tok16[...]
    outgoing = jnp.dot(select.astype(BF16), tokens16, preferred_element_type=F32).astype(BF16)
    for i in range(slots // 2):
        msg[i] = outgoing[2 * i : 2 * i + 2, :]

    with jax.named_scope("w_barrier"):
        pl.semaphore_wait(barrier, 4 * close + 1 + nx - 1 + ny - 1)

    def tell(sem, d, core):
        pl.semaphore_signal(sem, inc=1, device_id=(at(d), core, y, x), device_id_type=MESH)

    tell(entered.at[0], -close, c)
    tell(entered.at[1], close, c)

    def bundle(first, count, landing, target, k):
        return pltpu.make_async_remote_copy(
            src_ref=msg.at[pl.ds(2 * (first - least), 2 * count)],
            dst_ref=landing.at[:, c],
            send_sem=disp_send,
            recv_sem=rel_recv.at[k],
            device_id=(target, 1, y, x),
            device_id_type=MESH,
        )

    def ring(source):
        place, step = source + ends[1], 2 * ends[1]
        return place // step - place // (3 * step) - place // (4 * step)

    def send_near(d, core):
        pltpu.make_async_remote_copy(
            src_ref=msg.at[2 * (d - least) + core],
            dst_ref=rx.at[2 * z + c],
            send_sem=disp_send,
            recv_sem=disp_recv.at[ring(z)],
            device_id=(at(d), core, y, x),
            device_id_type=MESH,
        ).start()

    def near_plus(i, carry):
        for core in range(2):
            send_near(hop - i, core)
        return carry

    def near_minus(i, carry):
        for core in range(2):
            send_near(i - hop, core)
        return carry

    with jax.named_scope("w_plus"):
        pl.semaphore_wait(entered.at[0], 1)
    bundle(hop + 1, n_plus, relay_p, at(hop), 0).start()
    with jax.named_scope("w_minus"):
        pl.semaphore_wait(entered.at[1], 1)

    @pl.when(c == 1)
    def _():
        tell(entered.at[2], -hop, 1)
        tell(entered.at[3], hop, 1)

    bundle(least, n_minus, relay_m, at(-hop), 1).start()
    for i in range(1, ny):
        pl.semaphore_signal(entered.at[4], inc=1, device_id=in_column(i), device_id_type=MESH)
    lax.fori_loop(0, hop, near_plus, 0)
    lax.fori_loop(0, hop, near_minus, 0)
    send_near(0, 1 - c)
    rx[2 * z + c] = msg[c - 2 * least]

    def to_tp(src, dst, recv):
        def one(i, carry):
            j, device = peer(i)
            pltpu.make_async_remote_copy(
                src_ref=src(j),
                dst_ref=dst,
                send_sem=tp_send,
                recv_sem=recv,
                device_id=device,
                device_id_type=MESH,
            ).start()
            return carry

        lax.fori_loop(1, ntp, one, 0)

    def waiting(src, dst, send, recv):
        return pltpu.make_async_remote_copy(
            src_ref=src,
            dst_ref=dst,
            send_sem=send,
            recv_sem=recv,
            device_id=peer(1)[1],
            device_id_type=MESH,
        )

    gains = gain[...] * DOWN_SCALE
    values = tokens16.astype(F32)
    scaled_tok = (values * gains).astype(BF16)
    squares = row_of(jnp.sum(values * values, axis=1, keepdims=True), 128)
    for j in range(ntp):
        spart_tx[j, 16:24] = jnp.concatenate([squares, jnp.zeros((7, 128), F32)], axis=0)
    for i in (4, 5):
        loads[i].wait()
    for n, w in enumerate((sg, su)):
        part = jnp.dot(scaled_tok, w[...], preferred_element_type=F32)
        for k in range(ntp // 2):
            for h in range(2):
                spart_tx[2 * k + h, 8 * n : 8 * n + 8] = part[
                    8 * h : 8 * h + 8, k * chunk : (k + 1) * chunk
                ]
    spart_rx[me] = spart_tx[me]

    if ny > 1:
        pl.semaphore_wait(entered.at[4], ny - 1)
    slot_weight = slot_weight.T
    for i in range(3):
        term = slot_weight.astype(BF16)
        slotw[16 * i : 16 * i + 16, :] = term
        slot_weight = slot_weight - term.astype(F32)
    to_tp(lambda j: spart_tx.at[j], spart_rx.at[me], part_recv.at[groups])

    def forward(landing, i, source, first):
        for core in range(2):
            pltpu.make_async_remote_copy(
                src_ref=landing.at[2 * i + core],
                dst_ref=rx.at[pl.ds(2 * source, 2)],
                send_sem=rel_send,
                recv_sem=disp_recv.at[ring(source)],
                device_id=(at(first + i), core, y, x),
                device_id_type=MESH,
            ).start()

    def relay_up():
        with jax.named_scope("w_entered"):
            pl.semaphore_wait(entered.at[2], 1)
        with jax.named_scope("w_relp"):
            waiting(relay_p, relay_p, rel_send, rel_recv.at[0]).wait_recv()

        def one(k, carry):
            forward(relay_p, n_plus - 1 - k, at(-hop), 1)
            return carry

        lax.fori_loop(0, n_plus, one, 0)

    def relay_down():
        with jax.named_scope("w_entered"):
            pl.semaphore_wait(entered.at[3], 1)
        with jax.named_scope("w_relm"):
            waiting(relay_m, relay_m, rel_send, rel_recv.at[1]).wait_recv()

        def one(i, carry):
            forward(relay_m, i, at(hop), hop + least)
            return carry

        lax.fori_loop(0, n_minus, one, 0)

    @pl.when(jnp.logical_and(c == 1, z < nz - hop))
    def _():
        relay_up()
        relay_down()

    @pl.when(jnp.logical_and(c == 1, z >= nz - hop))
    def _():
        relay_down()
        relay_up()

    def gate_up(group):
        first, last = 2 * ends[group], 2 * ends[group + 1]
        rows = 2 * (last - first)
        half = rows // 2
        mine = ring(z) == group
        with jax.named_scope(f"w_rows{group}"):
            for count, there in ((last - first - 1, mine), (last - first, jnp.logical_not(mine))):
                arrived = rx.at[pl.ds(first, count)]

                @pl.when(there)
                def _():
                    waiting(arrived, arrived, disp_send, disp_recv.at[group]).wait_recv()

        values = rx[first:last].reshape(rows, width).astype(F32)
        lhs = (values * gains).astype(BF16)
        for n, w in enumerate((eg, eu)):
            part = jnp.dot(lhs, w[...], preferred_element_type=F32).astype(BF16)
            for k in range(ntp // 2):
                for h in range(2):
                    part_tx[group][2 * k + h, half * n : half * (n + 1)] = part[
                        half * h : half * (h + 1), k * chunk : (k + 1) * chunk
                    ]
        squares = row_of(jnp.sum(values * values, axis=1, keepdims=True), 128)
        terms = jnp.concatenate([*three_terms(squares), jnp.zeros((5, 128), BF16)], axis=0)
        for j in range(ntp):
            part_tx[group][j, 2 * half : 2 * half + 8] = terms

    def scatter(group):
        to_tp(lambda j: part_tx[group].at[j], part_rx[group].at[me], part_recv.at[group])
        part_rx[group][me] = part_tx[group][me]

    def hidden_of(parts, n):
        gate = jnp.zeros((n, chunk), F32)
        up = jnp.zeros((n, chunk), F32)
        total = jnp.zeros((8, 128), F32)
        for j in range(ntp):
            gate = gate + parts[j, 0:n].astype(F32)
            up = up + parts[j, n : 2 * n].astype(F32)
            total = total + parts[j, 2 * n : 2 * n + 8].astype(F32)
        total = total[0:1] + (total[1:2] + total[2:3])
        inv = lax.rsqrt(total / total_width + 1e-06) * UP_SCALE
        inv = col_of(inv, n, my_half * n)
        return (silu(gate * inv) * (up * inv)).astype(BF16)

    def tp_wait(buf, recv):
        some = buf.at[pl.ds(0, ntp - 1)]
        waiting(some, some, tp_send, recv).wait_recv()

    columns = pl.ds(pl.multiple_of(my_chunk * chunk, chunk), chunk)

    def reduce_group(group):
        half = 2 * (ends[group + 1] - ends[group])
        with jax.named_scope(f"w_rs{group}"):
            tp_wait(part_rx[group], part_recv.at[group])
        hid_tx[group][...] = hidden_of(part_rx[group], half)
        own = hid[group].at[my_half, :, columns]
        to_tp(lambda j: hid_tx[group], own, hid_recv.at[group])
        own[...] = hid_tx[group][...]

    shared_blocks = part_rx[groups - 1].at[pl.ds(0, ntp - 1), pl.ds(0, 8)]

    def reduce_shared():
        with jax.named_scope("w_rss"):
            tp_wait(spart_rx, part_recv.at[groups])
        shid_tx[...] = hidden_of(spart_rx, 8)
        own = shid.at[my_half, :, columns]
        to_tp(lambda j: shid_tx, own, hid_recv.at[groups])
        own[...] = shid_tx[...]

    def down_shared():
        with jax.named_scope("w_ags"):
            waiting(shared_blocks, shared_blocks, tp_send, hid_recv.at[groups]).wait_recv()
        hidden = jnp.concatenate([shid[0], shid[1]], axis=0)
        shared_out[...] = jnp.dot(hidden, sd[...], preferred_element_type=F32)

    def give_back(source):
        place_there = 2 * lax.rem(z - source - least + nz, nz) + c
        for core in range(2):

            @pl.when(2 * source + core != 2 * z + c)
            def _():
                pltpu.make_async_remote_copy(
                    src_ref=ret.at[2 * source + core],
                    dst_ref=back.at[place_there],
                    send_sem=ret_send,
                    recv_sem=ret_recv,
                    device_id=(source, core, y, x),
                    device_id_type=MESH,
                ).start()

    def down(group):
        low, high = ends[group], ends[group + 1]
        rows = 4 * (high - low)
        blocks = part_rx[group].at[pl.ds(0, ntp - 1), pl.ds(0, rows // 2)]
        with jax.named_scope(f"w_ag{group}"):
            waiting(blocks, blocks, tp_send, hid_recv.at[group]).wait_recv()
        hidden = jnp.concatenate([hid[group][0], hid[group][1]], axis=0)
        result = jnp.dot(hidden, ed[...], preferred_element_type=F32)
        result = result.astype(BF16)
        for i in range(rows // 2):
            ret[2 * low + i] = result[2 * i : 2 * i + 2, :]

        def one(i, carry):
            give_back(low + i)
            return carry

        lax.fori_loop(0, high - low, one, 0)

    for i in (6, 7, 8, 9):
        loads[i].wait()
    reduce_shared()
    gate_up(0)
    scatter(0)
    gate_up(1)
    scatter(1)
    gate_up(2)
    down_shared()
    reduce_group(0)
    reduce_group(1)
    down(0)
    scatter(2)
    down(1)
    reduce_group(2)
    down(2)
    back[c - 2 * least] = ret[2 * z + c]

    got = back.at[pl.ds(0, 2 * nz - 1)]
    with jax.named_scope("w_back"):
        waiting(got, got, ret_send, ret_recv).wait_recv()
    terms = jnp.dot(
        slotw[...], back[...].reshape(slots, width), preferred_element_type=F32
    )
    routed = terms[0:16, :] + (terms[16:32, :] + terms[32:48, :])
    out_ref[...] = (shared_out[...] + routed)[0:tok_n, :].astype(BF16)

    def left(ref, sem):
        waiting(ref, ref, sem, ret_recv).wait_send()

    left(got, ret_send)
    left(msg.at[pl.ds(0, 2 * (n_plus + n_minus))], disp_send)
    left(msg.at[pl.ds(0, 4 * hop + 1)], disp_send)

    @pl.when(c == 1)
    def _():
        left(relay_p, rel_send)
        left(relay_m, rel_send)

    left(spart_rx.at[pl.ds(0, ntp - 1)], tp_send)
    left(shared_blocks, tp_send)
    for group in range(groups):
        left(part_rx[group].at[pl.ds(0, ntp - 1)], tp_send)
        half = 2 * (ends[group + 1] - ends[group])
        left(part_rx[group].at[pl.ds(0, ntp - 1), pl.ds(0, half)], tp_send)


def local(sizes, tokens, norm_gain, routes, route_weights, eg, eu, ed, sg, su, sd):
    nz, ny, nx, hop = sizes
    ntp = ny * nx
    tok_n, width = tokens.shape
    picks = routes.shape[1]
    ff = eg.shape[2]
    chunk = ff // (ntp // 2)
    slots = 4 * nz
    ends = rings(nz)
    groups = len(ends) - 1
    halves = [2 * (high - low) for low, high in zip(ends, ends[1:])]
    n_plus, n_minus = nz // 2 - hop, nz // 2 - 1 - hop
    vm, dma = pltpu.VMEM, pltpu.SemaphoreType.DMA
    scratch = [
        vm((tok_n, width), BF16),
        vm((1, width), F32),
        vm((picks, tok_n), jnp.int32),
        vm((picks, tok_n), F32),
        vm((width, ff), BF16),
        vm((width, ff), BF16),
        vm((ff, width), BF16),
        vm((width, ff), BF16),
        vm((width, ff), BF16),
        vm((ff, width), BF16),
        vm((16, width), BF16),
        vm((picks, 16), jnp.int32),
        vm((picks, 16), F32),
        vm((48, slots), BF16),
        vm((16, width), F32),
        vm((slots // 2, 2, width), BF16),
        vm((2 * n_plus, 2, 2, width), BF16),
        vm((2 * n_minus, 2, 2, width), BF16),
        vm((slots // 2, 2, width), BF16),
        vm((ntp, 24, chunk), F32),
        vm((ntp, 24, chunk), F32),
        vm((8, chunk), BF16),
        vm((2, 8, ff), BF16),
        [vm((2, half, ff), BF16) for half in halves],
        vm((slots // 2, 2, width), BF16),
        vm((slots // 2, 2, width), BF16),
        [vm((ntp, 2 * half + 8, chunk), BF16) for half in halves],
        [vm((ntp, 2 * half + 8, chunk), BF16) for half in halves],
        [vm((half, chunk), BF16) for half in halves],
        dma((10,)),
        dma,
        dma((groups,)),
        dma,
        dma((2,)),
        dma,
        dma((groups + 1,)),
        dma((groups + 1,)),
        dma,
        dma,
        pltpu.SemaphoreType.REGULAR((5,)),
    ]
    def held(a):
        return pltpu.with_memory_space_constraint(a, pltpu.HBM)

    return pl.pallas_call(
        functools.partial(kernel, sizes),
        out_shape=jax.ShapeDtypeStruct((tok_n, width), BF16),
        in_specs=[pl.BlockSpec(memory_space=pl.ANY)] * 10,
        out_specs=pl.BlockSpec(memory_space=pltpu.VMEM),
        scratch_shapes=scratch,
        compiler_params=pltpu.CompilerParams(collective_id=0, has_side_effects=True, vmem_limit_bytes=40 << 20),
        name="moe_step",
    )(*map(held, (tokens, norm_gain.reshape(1, width), routes.T, route_weights.T, eg, eu, ed, sg, su, sd)))


def on_torus(torus):
    n = torus.shape
    sizes = (n["z"], n["y"], n["x"], (3 * n["z"] + 14) // 16)
    ep, tp = ("z", "c"), ("y", "x")
    in_specs = (
        P(ep, tp),
        P(tp),
        P(ep, None),
        P(ep, None),
        P(ep, tp, None),
        P(ep, tp, None),
        P(ep, None, tp),
        P(tp, None),
        P(tp, None),
        P(None, tp),
    )
    return jax.shard_map(
        functools.partial(local, sizes),
        mesh=torus,
        in_specs=in_specs,
        out_specs=P(ep, tp),
        check_vma=False,
    )


def solution(mesh):
    return on_torus(Mesh(mesh.devices.reshape(32, 2, 4, 4), ("z", "c", "y", "x")))
```
